32 devices in a mesh: dp: 4 (over y, x), kv: 4 (over z), tp: 2 (over core).
Axes of the slice: x: 2, y: 2, z: 4, core: 2. Of those that a mesh axis runs over, the one named last changes fastest.
Arguments:
- tokens: bfloat16 [192, 2048], P(('dp', 'tp'), 'kv'), may hold values from -8 to 8
- mix_gain: float32 [2048], replicated, may hold values from 0.1 to 1.9
- w_gate: bfloat16 [2048, 4096], P(None, 'kv'), may hold values from -0.125 to 0.125
- w_value: bfloat16 [2048, 4096], P(None, 'kv'), may hold values from -0.125 to 0.125
- w_maps: bfloat16 [2048, 16384], P(None, 'kv'), may hold values from -0.125 to 0.125
- w_step: bfloat16 [2048, 64], replicated, may hold values from -0.125 to 0.125
- conv_value: float32 [4, 4096], P(None, 'kv'), may hold values from -0.5 to 0.5
- conv_maps: float32 [4, 16384], P(None, 'kv'), may hold values from -0.5 to 0.5
- past_value: bfloat16 [192, 3, 4096], P(('dp', 'tp'), None, 'kv'), may hold values from -6 to 6
- past_maps: bfloat16 [192, 3, 16384], P(('dp', 'tp'), None, 'kv'), may hold values from -6 to 6
- step_bias: float32 [64], P('kv'), may hold values from -3 to 0
- decay_log: float32 [64], P('kv'), may hold values from 0 to 2.77
- skip_gain: float32 [64], P('kv'), may hold values from 0.1 to 1.9
- head_gain: float32 [4096], P('kv'), may hold values from 0.1 to 1.9
- state: float32 [192, 64, 64, 128], P(('dp', 'tp'), 'kv'), may hold values from -2 to 2
- w_out: bfloat16 [4096, 2048], P('kv'), may hold values from -0.125 to 0.125
- mlp_gain: float32 [2048], replicated, may hold values from 0.1 to 1.9
- w_up: bfloat16 [2048, 8192], P(None, 'kv'), may hold values from -0.125 to 0.125
- w_down: bfloat16 [8192, 2048], P('kv'), may hold values from -0.09375 to 0.09375
Outputs:
- layer_out: bfloat16 [192, 2048], P(('dp', 'tp'), 'kv')
- state_next: float32 [192, 64, 64, 128], P(('dp', 'tp'), 'kv')
- value_tail: bfloat16 [192, 3, 4096], P(('dp', 'tp'), None, 'kv')
- maps_tail: bfloat16 [192, 3, 16384], P(('dp', 'tp'), None, 'kv')
The draws below stay inside these ranges and needn't reach their ends.
All inputs are finite; a program needn't handle non-finite values.
Results may differ from the reference program's by a relative error of at most 0.0081.
Values may be sent and summed in bfloat16 or wider, within the bound.
A program may use at most 128 MiB of HBM per device.

```python
import jax
import jax.numpy as jnp
from jax import lax

D = 2048
HEADS = 64
HEAD_DIM = 64
STATE = 128
GROUPS = 64
KERNEL = 4
FF = 8192
INNER = 4096
MAPS = 16384
BATCH = 192


def draw_tokens(key, part):
    streams = jax.random.split(jax.random.fold_in(key, 17), 4)
    columns = jnp.arange(D, dtype=jnp.float32)
    spread = jnp.exp(jax.random.uniform(streams[0], (D,), jnp.float32) * jnp.log(10.0))
    col_scale = spread * (1.0 + 3.0 * columns / D)
    col_scale = col_scale / jnp.sqrt(jnp.mean(col_scale * col_scale))
    noise_part = jax.random.normal(streams[1], (BATCH, D), jnp.float32)
    row_scale = jnp.exp(jax.random.uniform(streams[3], (BATCH, 1), jnp.float32, -0.35, 0.35))
    return jnp.clip(noise_part * col_scale[None, :] * row_scale, -8.0, 8.0).astype(jnp.bfloat16)


def with_spikes(result, stream_key, source, target, shards_of, factor):
    def block_of(position):
        return (jnp.arange(result.shape[position]) // (result.shape[position] // shards_of)).reshape((-1,) + (1,) * (result.ndim - 1 - position))

    near = jax.random.permutation(stream_key, shards_of)[block_of(target)]
    far = (block_of(target) + shards_of // 2) % shards_of
    return jnp.where((block_of(source) == near) | (block_of(source) == far), factor * result, result)


def block_levels(own_key, extent, cuts, least, largest):
    def one(position, shards_of):
        heights = jax.random.uniform(jax.random.fold_in(jax.random.fold_in(own_key, 6), position), (shards_of,), jnp.float32, least / len(cuts), largest / len(cuts))
        return jnp.repeat(jnp.exp(heights), extent[position] // shards_of).reshape((-1,) + (1,) * (len(extent) - position - 1))

    level = one(*cuts[0])
    for cut in cuts[1:]:
        level = level * one(*cut)
    return level


def noise(own_key, shape, scale, bound, cuts=(), kind=jnp.bfloat16):
    entries = jax.random.normal(own_key, shape, jnp.float32) * scale
    if len(cuts) > 0:
        entries = block_levels(own_key, shape, cuts, -0.22, 0.18) * entries
    return jnp.clip(entries, min=-bound, max=bound).astype(kind)


def heavy_noise(own_key, shape, deviation, limit, cuts, heavy, kind=jnp.bfloat16):
    entries = deviation * jax.random.normal(own_key, shape, jnp.float32)
    if cuts:
        entries = entries * block_levels(own_key, shape, cuts, -0.22, 0.18)
    return jnp.clip(with_spikes(entries, jax.random.fold_in(own_key, 3), *heavy), -limit, limit).astype(kind)


def setup_inputs(seed: int = 0) -> dict:
    streams_of = jax.random.split(jax.random.key(seed), 20)
    return {
        "tokens": draw_tokens(jax.random.fold_in(streams_of[19], 71), 0),
        "mix_gain": jnp.clip(1.0 + 0.18 * jax.random.normal(streams_of[1], (D,), jnp.float32), 0.1, 1.9),
        "w_gate": noise(streams_of[2], (D, INNER), D ** -0.5, 0.125, ((1, 4),)),
        "w_value": noise(streams_of[3], (D, INNER), D ** -0.5, 0.125, ((1, 4),)),
        "w_maps": noise(streams_of[4], (D, MAPS), D ** -0.5, 0.125, ((1, 4),)),
        "w_step": noise(streams_of[5], (D, HEADS), D ** -0.5, 0.125),
        "conv_value": jnp.clip(jax.random.uniform(streams_of[6], (KERNEL, INNER), jnp.float32, -0.5, 0.5) * block_levels(streams_of[6], (KERNEL, INNER), ((1, 4),), -0.4, 0.0), -0.5, 0.5),
        "conv_maps": jnp.clip(jax.random.uniform(streams_of[7], (KERNEL, MAPS), jnp.float32, -0.5, 0.5) * block_levels(streams_of[7], (KERNEL, MAPS), ((1, 4),), -0.4, 0.0), -0.5, 0.5),
        "past_value": noise(streams_of[8], (BATCH, KERNEL - 1, INNER), 1.0, 6.0, ((0, 8), (2, 4))),
        "past_maps": noise(streams_of[9], (BATCH, KERNEL - 1, MAPS), 1.0, 6.0, ((0, 8), (2, 4))),
        "step_bias": jnp.clip(-3.0 + 3.0 * jax.random.uniform(streams_of[10], (HEADS,), jnp.float32) ** block_levels(streams_of[10], (HEADS,), ((0, 4),), -0.2, 0.2), -3.0, 0.0),
        "decay_log": jnp.clip(2.77 * jax.random.uniform(streams_of[11], (HEADS,), jnp.float32) ** block_levels(streams_of[11], (HEADS,), ((0, 4),), -0.2, 0.2), 0.0, 2.77),
        "skip_gain": jnp.clip(1.0 + 0.18 * jax.random.normal(streams_of[12], (HEADS,), jnp.float32), 0.1, 1.9),
        "head_gain": jnp.clip(1.0 + 0.18 * jax.random.normal(streams_of[13], (INNER,), jnp.float32), 0.1, 1.9),
        "state": noise(streams_of[14], (BATCH, HEADS, HEAD_DIM, STATE), 0.3, 2.0, ((0, 8), (1, 4)), jnp.float32),
        "w_out": heavy_noise(streams_of[15], (INNER, D), INNER ** -0.5, 0.125, ((0, 4),), (0, 1, 4, 2.0)),
        "mlp_gain": jnp.clip(1.0 + 0.18 * jax.random.normal(streams_of[16], (D,), jnp.float32), 0.1, 1.9),
        "w_up": noise(streams_of[17], (D, FF), D ** -0.5, 0.125, ((1, 4),)),
        "w_down": heavy_noise(streams_of[18], (FF, D), FF ** -0.5, 0.09375, ((0, 4),), (0, 1, 4, 2.0)),
    }


NORM_EPS = 1e-05

def rms_rows(matrix, gain_vec):
    widened = matrix.astype(jnp.float32)
    inv_scale = lax.rsqrt(lax.optimization_barrier(jnp.mean(widened * widened, axis=-1, keepdims=True)) + NORM_EPS)
    return (widened * inv_scale * gain_vec).astype(jnp.bfloat16)

def short_conv(past_rows, newest, kernel):
    window = jnp.concatenate([past_rows, newest[:, None, :]], axis=1)
    summed = lax.optimization_barrier(jnp.sum(window.astype(jnp.float32) * kernel[None], axis=1))
    return (jax.nn.silu(summed), window[:, 1:, :])

def reference(tokens, mix_gain, w_gate, w_value, w_maps, w_step, conv_value, conv_maps, past_value, past_maps, step_bias, decay_log, skip_gain, head_gain, state, w_out, mlp_gain, w_up, w_down):
    normed = rms_rows(tokens, mix_gain)
    gate_pre = jnp.dot(normed, w_gate, preferred_element_type=jnp.float32)
    step_pre = jnp.dot(normed, w_step, preferred_element_type=jnp.float32)
    value_new = jnp.dot(normed, w_value, preferred_element_type=jnp.float32).astype(jnp.bfloat16)
    maps_new = jnp.dot(normed, w_maps, preferred_element_type=jnp.float32).astype(jnp.bfloat16)
    value_act, value_tail = short_conv(past_value, value_new, conv_value)
    maps_act, maps_tail = short_conv(past_maps, maps_new, conv_maps)
    rounded = lax.optimization_barrier(maps_act.astype(jnp.bfloat16))
    grouped = rounded.astype(jnp.float32).reshape(BATCH, GROUPS, 2, STATE)
    per_group = HEADS // GROUPS
    in_map = jnp.repeat(grouped[:, :, 0], per_group, axis=1)
    out_map = jnp.repeat(grouped[:, :, 1], per_group, axis=1)
    head_values = value_act.reshape(BATCH, HEADS, HEAD_DIM)
    step_size = jax.nn.softplus(step_pre + step_bias)
    decay_rate = jnp.exp(-step_size * jnp.exp(decay_log))
    written = (step_size[:, :, None] * head_values)[:, :, :, None] * in_map[:, :, None, :]
    state_next = decay_rate[:, :, None, None] * state + written
    read_out = lax.optimization_barrier(jnp.sum(state_next * out_map[:, :, None, :], axis=-1)) + skip_gain[None, :, None] * head_values
    gated_heads = read_out * jax.nn.silu(gate_pre.reshape(BATCH, HEADS, HEAD_DIM))
    inv_scale = lax.rsqrt(lax.optimization_barrier(jnp.mean(gated_heads * gated_heads, axis=-1, keepdims=True)) + NORM_EPS)
    heads_out = (gated_heads * inv_scale * head_gain.reshape(HEADS, HEAD_DIM)).reshape(BATCH, INNER)
    heads_out = heads_out.astype(jnp.bfloat16)
    mixer_out = jnp.dot(heads_out, w_out, preferred_element_type=jnp.float32)
    hidden = lax.optimization_barrier((tokens.astype(jnp.float32) + mixer_out).astype(jnp.bfloat16))
    normed_mlp = rms_rows(hidden, mlp_gain)
    squared = jnp.square(jax.nn.relu(jnp.dot(normed_mlp, w_up, preferred_element_type=jnp.float32)))
    squared = squared.astype(jnp.bfloat16)
    layer_out = hidden.astype(jnp.float32) + jnp.dot(squared, w_down, preferred_element_type=jnp.float32)
    return (layer_out.astype(jnp.bfloat16), state_next, value_tail, maps_tail)
```

```python
import functools

import jax
import jax.numpy as jnp
from jax import lax
from jax.experimental import pallas as pl
from jax.experimental.pallas import tpu as pltpu
from jax.sharding import PartitionSpec as P

HEAD_DIM = 64
STATE = 128
MESH = pl.DeviceIdType.MESH


NORM_EPS = 1e-05
NT = (((1,), (1,)), ((), ()))


def partner(me, d):
    other = me
    bit = 1
    while bit <= d:
        if d & bit:
            other = other + bit - 2 * bit * lax.rem(lax.div(me, bit), 2)
        bit *= 2
    return other


def greet(peers, me):
    for d in range(1, peers):
        pl.semaphore_signal(
            pltpu.get_barrier_semaphore(),
            inc=1,
            device_id={"kv": partner(me, d)},
            device_id_type=MESH,
        )


def all_here(peers):
    pl.semaphore_wait(pltpu.get_barrier_semaphore(), peers - 1)


def far_first(peers):
    return list(range(1, peers))[::-1]


def push(src, dst, send_sem, recv_sem, target):
    return pltpu.make_async_remote_copy(
        src_ref=src,
        dst_ref=dst,
        send_sem=send_sem,
        recv_sem=recv_sem,
        device_id={"kv": target},
        device_id_type=MESH,
    )


def in_hbm(*arrays):
    return [pltpu.with_memory_space_constraint(x, pltpu.HBM) for x in arrays]


def in_vmem(*arrays):
    return [pltpu.with_memory_space_constraint(x, pltpu.VMEM) for x in arrays]


def silu(x):
    return x * jax.nn.sigmoid(x)


def split(x):
    high = x.astype(jnp.bfloat16).astype(jnp.float32)
    return high, x - high


def project_kernel(
    peers,
    tokens_in,
    gain_in,
    w_step_in,
    bias_in,
    decay_log_in,
    skip_in,
    conv_value_in,
    conv_maps_in,
    w_gate,
    w_value,
    w_maps,
    past_value_in,
    past_maps_in,
    state_in,
    gate_out,
    direct_out,
    value_out,
    maps_out,
    act_out,
    spread_out,
    decay_out,
    past_value,
    past_maps,
    state_out,
    tokens,
    gain,
    w_step,
    bias,
    decay_log,
    skip,
    conv_value,
    conv_maps,
    slots,
    weights,
    acc,
    small_sem,
    w_sem,
    state_sem,
    send_sem,
    recv_sem,
):
    me = lax.axis_index("kv")
    rows, part = tokens.shape
    chunks, width = weights.shape[1], weights.shape[3]
    heads = bias.shape[1]
    inner = value_out.shape[1]
    pair = 2 * HEAD_DIM
    taps = past_value.shape[0]
    greet(peers, me)

    def place(d):
        return pl.multiple_of(partner(me, d) * part, part)

    small = []
    for k, (src, dst) in enumerate(
        (
            (tokens_in, tokens),
            (gain_in, gain),
            (w_step_in, w_step),
            (bias_in, bias),
            (decay_log_in, decay_log),
            (skip_in, skip),
            (conv_value_in, conv_value),
            (conv_maps_in, conv_maps),
            (past_value_in, past_value),
            (past_maps_in, past_maps),
        )
    ):
        small.append(pltpu.make_async_copy(src, dst, small_sem.at[k]))
    def load_weights(d):
        for k, ref in enumerate((w_gate, w_value)):
            pltpu.make_async_copy(
                ref.at[pl.ds(place(d), part), :],
                weights.at[d, 0, :, pl.ds(k * inner, inner)],
                w_sem.at[d, 0],
            ).start(priority=1)
        for c in range(1, chunks):
            pltpu.make_async_copy(
                w_maps.at[pl.ds(place(d), part), pl.ds((c - 1) * width, width)],
                weights.at[d, c],
                w_sem.at[d, c],
            ).start(priority=1)

    for cp in small[:3]:
        cp.start()
    load_weights(0)
    small[0].wait()
    all_here(peers)
    sends = []
    for d in far_first(peers):
        cp = push(tokens, slots.at[d], send_sem.at[d], recv_sem.at[d], partner(me, d))
        cp.start()
        sends.append(cp)
    for cp in small[3:]:
        cp.start()
    for d in range(1, peers):
        load_weights(d)
    blocks = state_sem.shape[0]
    step_rows = rows // blocks
    state_copies = []
    for k in range(blocks):
        at = pl.ds(k * step_rows, step_rows)
        cp = pltpu.make_async_copy(state_in.at[at], state_out.at[at], state_sem.at[k])
        cp.start(priority=1)
        state_copies.append(cp)
    for cp in small[1:]:
        cp.wait()

    lane = lax.broadcasted_iota(jnp.int32, (rows, pair), 1)

    def by_head(table, h):
        return jnp.where(lane < HEAD_DIM, table[:, h : h + 1], table[:, h + 1 : h + 2])

    squares = jnp.zeros((rows, 1), jnp.float32)
    step_pre = jnp.zeros((2 * rows, w_step.shape[0]), jnp.float32)
    for d in range(peers):
        if d == 0:
            raw = tokens[...]
        else:
            push(tokens, slots.at[d], send_sem.at[d], recv_sem.at[d], me).wait_recv()
            raw = slots[d]
        wide = raw.astype(jnp.float32)
        squares = squares + jnp.sum(wide * wide, axis=1, keepdims=True)
        scaled = jnp.concatenate(split(wide * gain[:, pl.ds(place(d), part)]), axis=0)
        scaled = scaled.astype(jnp.bfloat16)
        step_pre = step_pre + lax.dot_general(
            scaled, w_step[:, pl.ds(place(d), part)], NT, preferred_element_type=jnp.float32
        )
        last = d == peers - 1
        if last:
            inv = lax.rsqrt(squares / (peers * part) + NORM_EPS)
            step_pre = (step_pre[:rows] + step_pre[rows:]) * inv
            own = step_pre[:, :heads]
            for j in range(1, peers):
                own = jnp.where(me == j, step_pre[:, j * heads : (j + 1) * heads], own)
            own = own + bias[...]
            step = jnp.maximum(own, 0.0) + jnp.log1p(jnp.exp(-jnp.abs(own)))
            decay = jnp.exp(-step * jnp.exp(decay_log[...]))
            for h in range(heads):
                decay_out[h] = jnp.broadcast_to(decay[:, h : h + 1], (rows, STATE))

        for c in range(chunks):
            pltpu.make_async_copy(
                w_maps.at[pl.ds(0, part), pl.ds(0, width)], weights.at[d, c], w_sem.at[d, c]
            ).wait()
            out = jnp.dot(scaled, weights[d, c], preferred_element_type=jnp.float32)
            out = out[:rows] + out[rows:]
            total = out if d == 0 else acc[c] + out
            if not last:
                acc[c] = total
                continue
            total = total * inv

            def conv(new, past, at, cols, table):
                summed = new.astype(jnp.float32) * table[taps : taps + 1, at : at + cols]
                for k in range(taps):
                    row = past[k, :, at : at + cols].astype(jnp.float32)
                    summed = summed + row * table[k : k + 1, at : at + cols]
                return silu(summed)

            if c == 0:
                gate_out[...] = silu(total[:, :inner])
                new = total[:, inner:].astype(jnp.bfloat16)
                value_out[...] = new
                act = conv(new, past_value, 0, inner, conv_value)
                for h in range(0, heads, 2):
                    at = h * HEAD_DIM
                    one = act[:, at : at + pair]
                    direct_out[:, at : at + pair] = by_head(skip, h) * one
                    one = one * by_head(step, h)
                    both = jnp.concatenate(split(one), axis=0)
                    blank = jnp.zeros((STATE - 4 * rows, HEAD_DIM), jnp.float32)
                    stack = jnp.concatenate(
                        [both[:, :HEAD_DIM], both[:, HEAD_DIM:], blank], axis=0
                    )
                    spread_out[h // 2] = stack.T.astype(jnp.bfloat16)
            else:
                at = (c - 1) * width
                new = total.astype(jnp.bfloat16)
                maps_out[:, at : at + width] = new
                act = conv(new, past_maps, at, width, conv_maps)
                act_out[:, at : at + width] = act.astype(jnp.bfloat16)

    for cp in state_copies:
        cp.wait()
    for cp in sends:
        cp.wait_send()


def project(
    peers,
    tokens,
    mix_gain,
    w_step,
    step_bias,
    decay_log,
    skip_gain,
    conv_value,
    conv_maps,
    w_gate,
    w_value,
    w_maps,
    past_value,
    past_maps,
    state,
):
    rows, part = tokens.shape
    heads = step_bias.shape[0]
    inner, maps = w_value.shape[1], w_maps.shape[1]
    width = 2 * inner
    chunks = 1 + maps // width
    f32, bf16 = jnp.float32, jnp.bfloat16
    blocks = next(k for k in (8, 6, 4, 3, 2, 1) if rows % k == 0)
    vmem = pl.BlockSpec(memory_space=pltpu.VMEM)
    hbm = pl.BlockSpec(memory_space=pl.ANY)
    return pl.pallas_call(
        functools.partial(project_kernel, peers),
        out_shape=(
            pltpu.VMEM((rows, inner), f32),
            pltpu.VMEM((rows, inner), f32),
            pltpu.VMEM((rows, inner), bf16),
            pltpu.VMEM((rows, maps), bf16),
            pltpu.VMEM((rows, maps), bf16),
            pltpu.VMEM((heads // 2, HEAD_DIM, STATE), bf16),
            pltpu.VMEM((heads, rows, STATE), f32),
            pltpu.VMEM(past_value.shape, bf16),
            pltpu.VMEM(past_maps.shape, bf16),
            pltpu.VMEM(state.shape, f32),
        ),
        in_specs=[hbm] * 14,
        out_specs=(vmem,) * 10,
        scratch_shapes=[
            pltpu.VMEM((rows, part), bf16),
            pltpu.VMEM((1, peers * part), f32),
            pltpu.VMEM((w_step.shape[1], peers * part), bf16),
            pltpu.VMEM((1, heads), f32),
            pltpu.VMEM((1, heads), f32),
            pltpu.VMEM((1, heads), f32),
            pltpu.VMEM(conv_value.shape, f32),
            pltpu.VMEM(conv_maps.shape, f32),
            pltpu.VMEM((peers, rows, part), bf16),
            pltpu.VMEM((peers, chunks, part, width), bf16),
            pltpu.VMEM((chunks, rows, width), f32),
            pltpu.SemaphoreType.DMA((10,)),
            pltpu.SemaphoreType.DMA((peers, chunks)),
            pltpu.SemaphoreType.DMA((blocks,)),
            pltpu.SemaphoreType.DMA((peers,)),
            pltpu.SemaphoreType.DMA((peers,)),
        ],
        compiler_params=pltpu.CompilerParams(
            collective_id=0, has_side_effects=True, vmem_limit_bytes=28 * 1024 * 1024
        ),
        name="project",
    )(
        *in_hbm(
            tokens,
            mix_gain[None, :],
            w_step.T,
            step_bias[None, :],
            decay_log[None, :],
            skip_gain[None, :],
            conv_value,
            conv_maps,
            w_gate,
            w_value,
            w_maps,
            past_value,
            past_maps,
            state,
        )
    )


def state_kernel(
    gate,
    direct,
    value_new,
    maps_new,
    maps_act,
    spread,
    decay,
    past_value,
    past_maps,
    state,
    head_gain_in,
    w_out_in,
    heads_out,
    w_out,
    state_out,
    value_tail,
    maps_tail,
    fresh,
    pick,
    read,
    head_gain,
    in_sem,
    tail_sem,
    out_sem,
):
    rows, heads = state.shape[:2]
    taps = past_value.shape[0]
    pair = 2 * HEAD_DIM
    wide = 4 * STATE
    group = 4
    loads = [
        pltpu.make_async_copy(head_gain_in, head_gain, in_sem.at[0]),
        pltpu.make_async_copy(w_out_in, w_out, in_sem.at[1]),
    ]
    tails = []
    for k, (past, new, tail) in enumerate(
        ((past_value, value_new, value_tail), (past_maps, maps_new, maps_tail))
    ):
        tails.append(
            pltpu.make_async_copy(
                past.at[pl.ds(1, taps - 1)], tail.at[pl.ds(0, taps - 1)], tail_sem.at[k, 0]
            )
        )
        tails.append(pltpu.make_async_copy(new, tail.at[taps - 1], tail_sem.at[k, 1]))
    for cp in loads + tails:
        cp.start()

    lane = lax.broadcasted_iota(jnp.int32, (16, STATE), 1)
    for b in range(rows):
        hit = (lane == b) | (lane == rows + b) | (lane == 2 * rows + b) | (lane == 3 * rows + b)
        pick[b] = jnp.where(hit, 1.0, 0.0).astype(jnp.bfloat16)

    row = lax.broadcasted_iota(jnp.int32, (2 * rows, STATE), 0)
    lane = lax.broadcasted_iota(jnp.int32, (2 * rows, STATE), 1)
    seq = jnp.where(row >= rows, row - rows, row)
    owner = jnp.where((row >= rows) == (lane >= HEAD_DIM), seq, -1)

    def copy_out(i):
        at = pl.ds(2 * i, 2)
        return pltpu.make_async_copy(fresh.at[:, at], state_out.at[:, at], out_sem.at[i])

    def one_pair(i):
        maps = maps_act[:, pl.ds(pl.multiple_of(i * wide, wide), wide)].astype(jnp.float32)
        ins = []
        for hh in range(2):
            ins += [maps[:, 2 * hh * STATE : (2 * hh + 1) * STATE]] * 2
        blank = jnp.zeros((2 * rows, STATE), jnp.float32)
        none = jnp.zeros((STATE - 4 * rows, STATE), jnp.float32)
        left = jnp.concatenate(ins[:2] + [blank, none], axis=0)
        right = jnp.concatenate([blank] + ins[2:] + [none], axis=0)
        into = jnp.concatenate([left, right], axis=1).astype(jnp.bfloat16)
        readers = jnp.concatenate(
            [maps[:, STATE : 2 * STATE], maps[:, 3 * STATE :]], axis=0
        ).astype(jnp.bfloat16)
        values = spread[i]
        found_all = jnp.zeros((2 * rows, pair), jnp.float32)
        for b in range(0, rows, group):
            count = min(group, rows - b)
            chosen = jnp.concatenate(
                [values * jnp.concatenate([pick[b + k]] * (HEAD_DIM // 16), axis=0) for k in range(count)],
                axis=0,
            )
            written = jnp.dot(chosen, into, preferred_element_type=jnp.float32)
            for k0 in range(0, count, 2):
                news = []
                for k in range(k0, k0 + 2):
                    for hh in range(2):
                        h = 2 * i + hh
                        new = (
                            decay[h, pl.ds(b + k, 1), :] * state[b + k, h]
                            + written[
                                k * HEAD_DIM : (k + 1) * HEAD_DIM, hh * STATE : (hh + 1) * STATE
                            ]
                        )
                        fresh[b + k, h] = new
                        news.append(new.astype(jnp.bfloat16))
                found = lax.dot_general(
                    readers,
                    jnp.concatenate(news, axis=0),
                    NT,
                    preferred_element_type=jnp.float32,
                )
                for k in range(2):
                    found_all = found_all + jnp.where(
                        owner == b + k0 + k, found[:, k * pair : (k + 1) * pair], 0.0
                    )
        read[:, pl.ds(pl.multiple_of(i * pair, pair), pair)] = found_all[:rows] + found_all[rows:]

        @pl.when(i > 0)
        def _():
            copy_out(i - 1).start(priority=1)

    steps = 2 if (heads // 2) % 2 == 0 else 1

    def body(j, carry):
        for k in range(steps):
            one_pair(j * steps + k)
        return carry

    lax.fori_loop(0, heads // 2 // steps, body, 0)

    loads[0].wait()
    first = lax.broadcasted_iota(jnp.int32, (rows, pair), 1) < HEAD_DIM
    for i in range(heads // 2):
        at = slice(i * pair, (i + 1) * pair)
        gated = (read[:, at] + direct[:, at]) * gate[:, at]
        square = gated * gated
        low = jnp.sum(jnp.where(first, square, 0.0), axis=1, keepdims=True)
        top = jnp.sum(jnp.where(first, 0.0, square), axis=1, keepdims=True)
        inv = lax.rsqrt(jnp.where(first, low, top) / HEAD_DIM + NORM_EPS)
        heads_out[:, at] = (gated * inv * head_gain[:, at]).astype(jnp.bfloat16)
    copy_out(heads // 2 - 1).start(priority=1)
    loads[1].wait()
    for cp in tails:
        cp.wait()
    for i in range(heads // 2):
        copy_out(i).wait()


def step_state(parts, head_gain, w_out):
    state, past_v, past_m = parts[9], parts[7], parts[8]
    rows, heads = state.shape[:2]
    f32, bf16 = jnp.float32, jnp.bfloat16
    vmem = pl.BlockSpec(memory_space=pltpu.VMEM)
    hbm = pl.BlockSpec(memory_space=pl.ANY)
    return pl.pallas_call(
        state_kernel,
        out_shape=(
            pltpu.VMEM((rows, heads * HEAD_DIM), bf16),
            pltpu.VMEM(w_out.shape, bf16),
            pltpu.HBM(state.shape, f32),
            pltpu.HBM(past_v.shape, bf16),
            pltpu.HBM(past_m.shape, bf16),
        ),
        in_specs=[vmem] * 10 + [hbm] * 2,
        out_specs=(vmem, vmem, hbm, hbm, hbm),
        scratch_shapes=[
            pltpu.VMEM(state.shape, f32),
            pltpu.VMEM((rows, 16, STATE), bf16),
            pltpu.VMEM((rows, heads * HEAD_DIM), f32),
            pltpu.VMEM((1, heads * HEAD_DIM), f32),
            pltpu.SemaphoreType.DMA((2,)),
            pltpu.SemaphoreType.DMA((2, 2)),
            pltpu.SemaphoreType.DMA((heads // 2,)),
        ],
        compiler_params=pltpu.CompilerParams(vmem_limit_bytes=16 * 1024 * 1024),
        name="step_state",
    )(*in_vmem(*parts), *in_hbm(head_gain[None, :], w_out))


def mixer_kernel(
    peers,
    heads,
    out_w,
    tokens_in,
    gain_in,
    w_up,
    w_down,
    layer_out,
    tokens,
    gain,
    up_w,
    down_w,
    sums_a,
    land_a,
    own_hidden,
    hidden,
    squared,
    sums_b,
    land_b,
    small_sem,
    up_sem,
    down_sem,
    send_a,
    recv_a,
    send_h,
    recv_h,
    send_b,
    recv_b,
):
    me = lax.axis_index("kv")
    rows, part = tokens.shape

    def place(d):
        return pl.multiple_of(partner(me, d) * part, part)

    order = far_first(peers) + [0]
    greet(peers, me)
    small = [
        pltpu.make_async_copy(tokens_in, tokens, small_sem.at[0]),
        pltpu.make_async_copy(gain_in, gain, small_sem.at[1]),
    ]
    ups = [
        pltpu.make_async_copy(w_up.at[pl.ds(place(d), part), :], up_w.at[d], up_sem.at[d])
        for d in range(peers)
    ]
    downs = [
        pltpu.make_async_copy(w_down.at[:, pl.ds(place(d), part)], down_w.at[d], down_sem.at[d])
        for d in range(peers)
    ]
    for cp in small:
        cp.start()

    pending = []

    def scatter(left, weights, sums, land, send, recv, after=None):
        for d in order:
            piece = jnp.dot(left, weights(d), preferred_element_type=jnp.float32)
            if d == 0:
                total = piece
            else:
                sums[d] = piece.astype(jnp.bfloat16)
                if not pending:
                    all_here(peers)
                cp = push(sums.at[d], land.at[d], send.at[d], recv.at[d], partner(me, d))
                cp.start()
                pending.append(cp)
        if after is not None:
            after()
        for d in range(1, peers):
            push(sums.at[d], land.at[d], send.at[d], recv.at[d], me).wait_recv()
            total = total + land[d].astype(jnp.float32)
        return total

    def out_block(d):
        return out_w[:, pl.ds(place(d), part)]

    def down_block(d):
        downs[d].wait()
        return down_w[d]

    def load_later():
        for cp in ups:
            cp.start(priority=1)
        for d in order:
            downs[d].start(priority=1)

    total = scatter(heads[...], out_block, sums_a, land_a, send_a, recv_a, load_later)
    for cp in small:
        cp.wait()
    mine = (tokens[...].astype(jnp.float32) + total).astype(jnp.bfloat16)
    own_hidden[...] = mine
    for d in far_first(peers):
        cp = push(own_hidden, hidden.at[d], send_h.at[d], recv_h.at[d], partner(me, d))
        cp.start()
        pending.append(cp)

    squares = jnp.zeros((rows, 1), jnp.float32)
    up = None
    for d in range(peers):
        if d == 0:
            raw = mine
        else:
            push(own_hidden, hidden.at[d], send_h.at[d], recv_h.at[d], me).wait_recv()
            raw = hidden[d]
        wide = raw.astype(jnp.float32)
        squares = squares + jnp.sum(wide * wide, axis=1, keepdims=True)
        scaled = jnp.concatenate(split(wide * gain[:, pl.ds(place(d), part)]), axis=0)
        ups[d].wait()
        out = jnp.dot(
            scaled.astype(jnp.bfloat16), up_w[d], preferred_element_type=jnp.float32
        )
        out = out[:rows] + out[rows:]
        up = out if d == 0 else up + out

    inv = lax.rsqrt(squares / (peers * part) + NORM_EPS)
    up = jnp.maximum(up * inv, 0.0)
    squared[...] = (up * up).astype(jnp.bfloat16)
    total = scatter(squared[...], down_block, sums_b, land_b, send_b, recv_b)
    layer_out[...] = (mine.astype(jnp.float32) + total).astype(jnp.bfloat16)
    for cp in pending:
        cp.wait_send()


def mix_channels(peers, heads_out, out_w, tokens, mlp_gain, w_up, w_down):
    rows, part = tokens.shape
    inner, hid = out_w.shape[0], w_up.shape[1]
    f32, bf16 = jnp.float32, jnp.bfloat16
    vmem = pl.BlockSpec(memory_space=pltpu.VMEM)
    hbm = pl.BlockSpec(memory_space=pl.ANY)
    sems = pltpu.SemaphoreType.DMA((peers,))
    slots = pltpu.VMEM((peers, rows, part), bf16)
    return pl.pallas_call(
        functools.partial(mixer_kernel, peers),
        out_shape=jax.ShapeDtypeStruct((rows, part), bf16),
        in_specs=[vmem] * 2 + [hbm] * 4,
        out_specs=vmem,
        scratch_shapes=[
            pltpu.VMEM((rows, part), bf16),
            pltpu.VMEM((1, peers * part), f32),
            pltpu.VMEM((peers, part, hid), bf16),
            pltpu.VMEM((peers, hid, part), bf16),
            slots,
            slots,
            pltpu.VMEM((rows, part), bf16),
            slots,
            pltpu.VMEM((rows, hid), bf16),
            slots,
            slots,
            pltpu.SemaphoreType.DMA((2,)),
            sems,
            sems,
            sems,
            sems,
            sems,
            sems,
            sems,
            sems,
        ],
        compiler_params=pltpu.CompilerParams(
            collective_id=1, has_side_effects=True, vmem_limit_bytes=24 * 1024 * 1024
        ),
        name="mix_channels",
    )(*in_vmem(heads_out, out_w), *in_hbm(tokens, mlp_gain[None, :], w_up, w_down))


def local_kernels(
    peers,
    tokens,
    mix_gain,
    w_gate,
    w_value,
    w_maps,
    w_step,
    conv_value,
    conv_maps,
    past_value,
    past_maps,
    step_bias,
    decay_log,
    skip_gain,
    head_gain,
    state,
    w_out,
    mlp_gain,
    w_up,
    w_down,
):
    parts = project(
        peers,
        tokens,
        mix_gain,
        w_step,
        step_bias,
        decay_log,
        skip_gain,
        conv_value,
        conv_maps,
        w_gate,
        w_value,
        w_maps,
        jnp.swapaxes(past_value, 0, 1),
        jnp.swapaxes(past_maps, 0, 1),
        state,
    )
    heads_out, out_w, state_next, tail_v, tail_m = step_state(parts, head_gain, w_out)
    layer_out = mix_channels(peers, heads_out, out_w, tokens, mlp_gain, w_up, w_down)
    return layer_out, state_next, jnp.swapaxes(tail_v, 0, 1), jnp.swapaxes(tail_m, 0, 1)


def kernels_fit(peers, tokens, state, w_maps, w_up):
    rows, part = tokens.shape
    heads = state.shape[1]
    inner = heads * HEAD_DIM
    weights = 2 * tokens.shape[1] * peers * (2 * inner + w_maps.shape[1])
    held = 4 * rows * heads * HEAD_DIM * STATE
    later = 2 * part * peers * (inner + 2 * w_up.shape[1])
    mib = 1024 * 1024
    return (
        peers > 1
        and peers & (peers - 1) == 0
        and rows % 8 == 0
        and 4 * rows <= STATE
        and part % 128 == 0
        and heads % 2 == 0
        and w_maps.shape[1] == heads * 2 * STATE
        and w_up.shape[1] % 128 == 0
        and weights + held <= 40 * mib
        and 2 * held + 2 * part * peers * inner <= 40 * mib
        and later <= 40 * mib
    )


def rms_rows(matrix, gain_vec):
    widened = matrix.astype(jnp.float32)
    inv_scale = lax.rsqrt(jnp.mean(widened * widened, axis=-1, keepdims=True) + NORM_EPS)
    return (widened * inv_scale * gain_vec).astype(jnp.bfloat16)


def short_conv(past_rows, newest, kernel):
    window = jnp.concatenate([past_rows, newest[:, None, :]], axis=1)
    summed = jnp.sum(window.astype(jnp.float32) * kernel[None], axis=1)
    return (jax.nn.silu(summed), window[:, 1:, :])


def local(
    tokens,
    mix_gain,
    w_gate,
    w_value,
    w_maps,
    w_step,
    conv_value,
    conv_maps,
    past_value,
    past_maps,
    step_bias,
    decay_log,
    skip_gain,
    head_gain,
    state,
    w_out,
    mlp_gain,
    w_up,
    w_down,
):
    whole_rows = lax.all_gather(tokens, "kv", axis=1, tiled=True)
    batch_rows = whole_rows.shape[0]
    heads_here = state.shape[1]
    head_start = lax.axis_index("kv") * heads_here
    normed = rms_rows(whole_rows, mix_gain)
    gate_pre = jnp.dot(normed, w_gate, preferred_element_type=jnp.float32)
    step_cols = lax.dynamic_slice_in_dim(w_step, head_start, heads_here, 1)
    step_pre = jnp.dot(normed, step_cols, preferred_element_type=jnp.float32)
    value_new = jnp.dot(normed, w_value, preferred_element_type=jnp.float32).astype(jnp.bfloat16)
    maps_new = jnp.dot(normed, w_maps, preferred_element_type=jnp.float32).astype(jnp.bfloat16)
    value_act, value_tail = short_conv(past_value, value_new, conv_value)
    maps_act, maps_tail = short_conv(past_maps, maps_new, conv_maps)
    maps_act = lax.optimization_barrier(maps_act.astype(jnp.bfloat16))
    grouped = maps_act.astype(jnp.float32).reshape(batch_rows, -1, 2, STATE)
    per_group = heads_here // grouped.shape[1]
    in_map = jnp.repeat(grouped[:, :, 0], per_group, axis=1)
    out_map = jnp.repeat(grouped[:, :, 1], per_group, axis=1)
    head_values = value_act.reshape(batch_rows, heads_here, HEAD_DIM)
    step_size = jax.nn.softplus(step_pre + step_bias)
    decay_rate = jnp.exp(-step_size * jnp.exp(decay_log))
    written = (step_size[:, :, None] * head_values)[:, :, :, None] * in_map[:, :, None, :]
    state_next = decay_rate[:, :, None, None] * state + written
    read_out = (
        jnp.sum(state_next * out_map[:, :, None, :], axis=-1)
        + skip_gain[None, :, None] * head_values
    )
    gated_heads = read_out * jax.nn.silu(gate_pre.reshape(batch_rows, heads_here, HEAD_DIM))
    inv_scale = lax.rsqrt(jnp.mean(gated_heads * gated_heads, axis=-1, keepdims=True) + NORM_EPS)
    heads_out = gated_heads * inv_scale * head_gain.reshape(heads_here, HEAD_DIM)
    heads_out = heads_out.reshape(batch_rows, heads_here * HEAD_DIM).astype(jnp.bfloat16)
    partial_value = jnp.dot(heads_out, w_out, preferred_element_type=jnp.float32)
    own_part = lax.psum_scatter(partial_value, "kv", scatter_dimension=1, tiled=True)
    own_hidden = lax.optimization_barrier(
        (tokens.astype(jnp.float32) + own_part).astype(jnp.bfloat16)
    )
    hidden = lax.all_gather(own_hidden, "kv", axis=1, tiled=True)
    normed_mlp = rms_rows(hidden, mlp_gain)
    squared = jnp.square(jax.nn.relu(jnp.dot(normed_mlp, w_up, preferred_element_type=jnp.float32)))
    squared = squared.astype(jnp.bfloat16)
    partial_mlp = jnp.dot(squared, w_down, preferred_element_type=jnp.float32)
    mlp_part = lax.psum_scatter(partial_mlp, "kv", scatter_dimension=1, tiled=True)
    layer_out = (own_hidden.astype(jnp.float32) + mlp_part).astype(jnp.bfloat16)
    return (layer_out, state_next, value_tail, maps_tail)


def solution(mesh):
    in_specs = (
        P(("dp", "tp"), "kv"),
        P(),
        P(None, "kv"),
        P(None, "kv"),
        P(None, "kv"),
        P(),
        P(None, "kv"),
        P(None, "kv"),
        P(("dp", "tp"), None, "kv"),
        P(("dp", "tp"), None, "kv"),
        P("kv"),
        P("kv"),
        P("kv"),
        P("kv"),
        P(("dp", "tp"), "kv", None, None),
        P("kv", None),
        P(),
        P(None, "kv"),
        P("kv", None),
    )
    out_specs = (
        P(("dp", "tp"), "kv"),
        P(("dp", "tp"), "kv", None, None),
        P(("dp", "tp"), None, "kv"),
        P(("dp", "tp"), None, "kv"),
    )
    peers = mesh.shape["kv"]

    def device_part(*args):
        if kernels_fit(peers, args[0], args[14], args[4], args[17]):
            return local_kernels(peers, *args)
        return local(*args)

    return jax.shard_map(
        device_part, mesh=mesh, in_specs=in_specs, out_specs=out_specs, check_vma=False
    )
```

```python
import functools

import jax
import jax.numpy as jnp
from jax import lax
from jax.experimental import pallas as pl
from jax.experimental.pallas import tpu as pltpu
from jax.sharding import PartitionSpec as P

HEAD_DIM = 64
STATE = 128
MESH = pl.DeviceIdType.MESH
FUSED_LIMIT = 49 * 1024 * 1024
WINDOW = 9


NORM_EPS = 1e-05
NT = (((1,), (1,)), ((), ()))


def partner(me, d):
    other = me
    bit = 1
    while bit <= d:
        if d & bit:
            other = other + bit - 2 * bit * lax.rem(lax.div(me, bit), 2)
        bit *= 2
    return other


def greet(peers, me):
    for d in range(1, peers):
        pl.semaphore_signal(
            pltpu.get_barrier_semaphore(),
            inc=1,
            device_id={"kv": partner(me, d)},
            device_id_type=MESH,
        )


def all_here(peers):
    pl.semaphore_wait(pltpu.get_barrier_semaphore(), peers - 1)


def far_first(peers):
    return list(range(1, peers))[::-1]


def push(src, dst, send_sem, recv_sem, target):
    return pltpu.make_async_remote_copy(
        src_ref=src,
        dst_ref=dst,
        send_sem=send_sem,
        recv_sem=recv_sem,
        device_id={"kv": target},
        device_id_type=MESH,
    )


def in_hbm(*arrays):
    return [pltpu.with_memory_space_constraint(x, pltpu.HBM) for x in arrays]


def in_vmem(*arrays):
    return [pltpu.with_memory_space_constraint(x, pltpu.VMEM) for x in arrays]


def silu(x):
    return x * jax.nn.sigmoid(x)


def split(x):
    high = x.astype(jnp.bfloat16).astype(jnp.float32)
    return high, x - high


def decode_kernel(
    peers,
    tokens_in,
    gain_in,
    w_step_in,
    bias_in,
    decay_log_in,
    skip_in,
    head_gain_in,
    mlp_gain_in,
    conv_value_in,
    conv_maps_in,
    past_value_in,
    past_maps_in,
    w_gate,
    w_value,
    w_maps,
    state_in,
    w_out,
    w_up,
    w_down,
    layer_out,
    value_new,
    maps_new,
    past_value,
    past_maps,
    state,
    tokens,
    gain,
    w_step,
    bias,
    decay_log,
    skip,
    head_gain,
    mlp_gain,
    conv_value,
    conv_maps,
    slots,
    weights,
    acc,
    gate,
    value_act,
    maps_act,
    decay_rows,
    step_cols,
    spread,
    pick,
    readers,
    read,
    out_w,
    up_w,
    down_w,
    sums_a,
    land_a,
    own_hidden,
    hidden,
    squared,
    sums_b,
    land_b,
    small_sem,
    w_sem,
    state_sem,
    out_sem,
    up_sem,
    down_sem,
    send_t,
    recv_t,
    send_a,
    recv_a,
    send_h,
    recv_h,
    send_b,
    recv_b,
):
    me = lax.axis_index("kv")
    rows, part = tokens.shape
    chunks, width = weights.shape[1], weights.shape[3]
    heads = bias.shape[1]
    inner = value_new.shape[1]
    pair = 2 * HEAD_DIM
    wide = 4 * STATE
    taps = past_value.shape[0]
    pairs = heads // 2
    greet(peers, me)

    def place(d):
        return pl.multiple_of(partner(me, d) * part, part)

    small = [
        pltpu.make_async_copy(src, dst, small_sem.at[k])
        for k, (src, dst) in enumerate(
            (
                (tokens_in, tokens),
                (gain_in, gain),
                (w_step_in, w_step),
                (bias_in, bias),
                (decay_log_in, decay_log),
                (skip_in, skip),
                (head_gain_in, head_gain),
                (mlp_gain_in, mlp_gain),
                (conv_value_in, conv_value),
                (conv_maps_in, conv_maps),
                (past_value_in, past_value),
                (past_maps_in, past_maps),
            )
        )
    ]

    def weight_copies(d, c):
        if c == 0:
            return [
                pltpu.make_async_copy(
                    ref.at[pl.ds(place(d), part), :],
                    weights.at[d, 0, :, pl.ds(k * inner, inner)],
                    w_sem.at[d, 0],
                )
                for k, ref in enumerate((w_gate, w_value))
            ]
        return [
            pltpu.make_async_copy(
                w_maps.at[pl.ds(place(d), part), pl.ds((c - 1) * width, width)],
                weights.at[d, c],
                w_sem.at[d, c],
            )
        ]

    blocks = state_sem.shape[0]
    block = rows // blocks

    def state_copy(r):
        at = pl.ds(r * block, block)
        return pltpu.make_async_copy(state_in.at[at], state.at[at], state_sem.at[r])

    order = far_first(peers) + [0]
    outs = [
        pltpu.make_async_copy(w_out.at[:, pl.ds(place(d), part)], out_w.at[d], out_sem.at[d])
        for d in range(peers)
    ]
    ups = [
        pltpu.make_async_copy(w_up.at[pl.ds(place(d), part), :], up_w.at[d], up_sem.at[d])
        for d in range(peers)
    ]
    downs = [
        pltpu.make_async_copy(w_down.at[:, pl.ds(place(d), part)], down_w.at[d], down_sem.at[d])
        for d in range(peers)
    ]
    bulk = [weight_copies(d, c) for d in range(peers) for c in range(chunks)]
    bulk += [[state_copy(r)] for r in range(blocks)] + [[outs[d]] for d in order]

    def load(count):
        for _ in range(min(count, len(bulk))):
            for cp in bulk.pop(0):
                cp.start(priority=1)

    for cp in small[:3]:
        cp.start()
    load(chunks)
    small[0].wait()
    all_here(peers)
    pending = []

    def send(src, dst, send_sem, recv_sem, d):
        cp = push(src, dst, send_sem.at[d], recv_sem.at[d], partner(me, d))
        cp.start()
        pending.append(cp)

    def arrived(src, dst, send_sem, recv_sem, d):
        push(src, dst, send_sem.at[d], recv_sem.at[d], me).wait_recv()

    for d in far_first(peers):
        send(tokens, slots.at[d], send_t, recv_t, d)
    for cp in small[3:]:
        cp.start()
    load(WINDOW - chunks)
    for cp in small[1:]:
        cp.wait()

    lane = lax.broadcasted_iota(jnp.int32, (rows, pair), 1)

    def by_head(table, h):
        return jnp.where(lane < HEAD_DIM, table[:, h : h + 1], table[:, h + 1 : h + 2])

    squares = jnp.zeros((rows, 1), jnp.float32)
    step_pre = jnp.zeros((2 * rows, w_step.shape[0]), jnp.float32)
    for d in range(peers):
        if d == 0:
            raw = tokens[...]
        else:
            arrived(tokens, slots.at[d], send_t, recv_t, d)
            raw = slots[d]
        x = raw.astype(jnp.float32)
        squares = squares + jnp.sum(x * x, axis=1, keepdims=True)
        scaled = jnp.concatenate(split(x * gain[:, pl.ds(place(d), part)]), axis=0)
        scaled = scaled.astype(jnp.bfloat16)
        step_pre = step_pre + lax.dot_general(
            scaled, w_step[:, pl.ds(place(d), part)], NT, preferred_element_type=jnp.float32
        )
        last = d == peers - 1
        if last:
            inv = lax.rsqrt(squares / (peers * part) + NORM_EPS)
            step_pre = (step_pre[:rows] + step_pre[rows:]) * inv
            own = step_pre[:, :heads]
            for j in range(1, peers):
                own = jnp.where(me == j, step_pre[:, j * heads : (j + 1) * heads], own)
            own = own + bias[...]
            step = jnp.maximum(own, 0.0) + jnp.log1p(jnp.exp(-jnp.abs(own)))
            decay = jnp.exp(-step * jnp.exp(decay_log[...]))
            for h in range(heads):
                decay_rows[h] = jnp.broadcast_to(decay[:, h : h + 1], (rows, STATE))
            for h in range(0, heads, 2):
                step_cols[:, h * HEAD_DIM : (h + 2) * HEAD_DIM] = by_head(step, h)

        for c in range(chunks):
            pltpu.make_async_copy(
                w_maps.at[pl.ds(0, part), pl.ds(0, width)], weights.at[d, c], w_sem.at[d, c]
            ).wait()
            load(1)
            out = jnp.dot(scaled, weights[d, c], preferred_element_type=jnp.float32)
            out = out[:rows] + out[rows:]
            total = out if d == 0 else acc[c] + out
            if not last:
                acc[c] = total
                continue
            total = total * inv

            def conv(new, past, at, cols, table):
                summed = new.astype(jnp.float32) * table[taps : taps + 1, at : at + cols]
                for k in range(taps):
                    row = past[k, :, at : at + cols].astype(jnp.float32)
                    summed = summed + row * table[k : k + 1, at : at + cols]
                return silu(summed)

            if c == 0:
                gate[...] = silu(total[:, :inner])
                new = total[:, inner:].astype(jnp.bfloat16)
                value_new[...] = new
                value_act[...] = conv(new, past_value, 0, inner, conv_value)
            else:
                at = (c - 1) * width
                new = total.astype(jnp.bfloat16)
                maps_new[:, at : at + width] = new
                act = conv(new, past_maps, at, width, conv_maps)
                maps_act[:, at : at + width] = act.astype(jnp.bfloat16)

    row = lax.broadcasted_iota(jnp.int32, (2 * rows, STATE), 0)
    column = lax.broadcasted_iota(jnp.int32, (2 * rows, STATE), 1)
    seq = jnp.where(row >= rows, row - rows, row)
    owner = jnp.where((row >= rows) == (column >= HEAD_DIM), seq, -1)
    read[...] = jnp.zeros_like(read)

    for i in range(pairs):
        at = i * wide
        readers[i] = jnp.concatenate(
            [
                maps_act[:, at + STATE : at + 2 * STATE].astype(jnp.float32),
                maps_act[:, at + 3 * STATE : at + wide].astype(jnp.float32),
            ],
            axis=0,
        ).astype(jnp.bfloat16)

    def read_pair(i, r):
        total = read[i]
        for k0 in range(0, block, 2):
            tiles = []
            for k in range(k0, k0 + 2):
                for hh in range(2):
                    tiles.append(state[r * block + k, 2 * i + hh].astype(jnp.bfloat16))
            found = lax.dot_general(
                readers[i], jnp.concatenate(tiles, axis=0), NT, preferred_element_type=jnp.float32
            )
            for k in range(2):
                total = total + jnp.where(
                    owner == r * block + k0 + k, found[:, k * pair : (k + 1) * pair], 0.0
                )
        read[i] = total

    for r in range(blocks):
        state_copy(r).wait()
        load(1)
        for i in range(pairs):
            read_pair(i, r)
    load(len(bulk))

    heads_out = []
    first = lane < HEAD_DIM
    for i in range(pairs):
        at = slice(i * pair, (i + 1) * pair)
        act = value_act[:, at]
        scaled = act * step_cols[:, at]
        inner_dots = []
        for hh in range(2):
            m = i * wide + 2 * hh * STATE
            into = maps_act[:, m : m + STATE].astype(jnp.float32)
            outof = maps_act[:, m + STATE : m + 2 * STATE].astype(jnp.float32)
            inner_dots.append(jnp.sum(into * outof, axis=1, keepdims=True))
        h = 2 * i
        decayed = jnp.where(first, decay_rows[h], decay_rows[h + 1])
        found = read[i]
        read_out = decayed * (found[:rows] + found[rows:])
        read_out = read_out + jnp.where(first, inner_dots[0], inner_dots[1]) * scaled
        gated = (read_out + by_head(skip, h) * act) * gate[:, at]
        square = gated * gated
        low = jnp.sum(jnp.where(first, square, 0.0), axis=1, keepdims=True)
        top = jnp.sum(jnp.where(first, 0.0, square), axis=1, keepdims=True)
        norm = lax.rsqrt(jnp.where(first, low, top) / HEAD_DIM + NORM_EPS)
        heads_out.append((gated * norm * head_gain[:, at]).astype(jnp.bfloat16))
    heads_out = jnp.concatenate(heads_out, axis=1)

    def scatter(left, waits, weight, sums, land, send_sem, recv_sem, between):
        for d in order:
            waits[d].wait()
            piece = jnp.dot(left, weight[d], preferred_element_type=jnp.float32)
            if d == 0:
                total = piece
            else:
                sums[d] = piece.astype(jnp.bfloat16)
                send(sums.at[d], land.at[d], send_sem, recv_sem, d)
        between()
        for d in range(1, peers):
            arrived(sums.at[d], land.at[d], send_sem, recv_sem, d)
            total = total + land[d].astype(jnp.float32)
        return total

    def prepare():
        spot = lax.broadcasted_iota(jnp.int32, (16, STATE), 1)
        for b in range(rows):
            hit = (spot == b) | (spot == rows + b)
            hit = hit | (spot == 2 * rows + b) | (spot == 3 * rows + b)
            pick[b] = jnp.where(hit, 1.0, 0.0).astype(jnp.bfloat16)
        blank = jnp.zeros((STATE - 4 * rows, HEAD_DIM), jnp.float32)
        for i in range(pairs):
            at = slice(i * pair, (i + 1) * pair)
            both = jnp.concatenate(split(value_act[:, at] * step_cols[:, at]), axis=0)
            stack = jnp.concatenate([both[:, :HEAD_DIM], both[:, HEAD_DIM:], blank], axis=0)
            spread[i] = stack.T.astype(jnp.bfloat16)

    def update(i, carry):
        maps = maps_act[:, pl.ds(pl.multiple_of(i * wide, wide), wide)].astype(jnp.float32)
        ins = []
        for hh in range(2):
            ins += [maps[:, 2 * hh * STATE : (2 * hh + 1) * STATE]] * 2
        blank = jnp.zeros((2 * rows, STATE), jnp.float32)
        none = jnp.zeros((STATE - 4 * rows, STATE), jnp.float32)
        left = jnp.concatenate(ins[:2] + [blank, none], axis=0)
        right = jnp.concatenate([blank] + ins[2:] + [none], axis=0)
        into = jnp.concatenate([left, right], axis=1).astype(jnp.bfloat16)
        values = spread[i]
        for b in range(0, rows, 4):
            chosen = jnp.concatenate(
                [
                    values * jnp.concatenate([pick[b + k]] * (HEAD_DIM // 16), axis=0)
                    for k in range(4)
                ],
                axis=0,
            )
            written = jnp.dot(chosen, into, preferred_element_type=jnp.float32)
            for k in range(4):
                for hh in range(2):
                    h = 2 * i + hh
                    state[b + k, h] = (
                        decay_rows[h, pl.ds(b + k, 1), :] * state[b + k, h]
                        + written[k * HEAD_DIM : (k + 1) * HEAD_DIM, hh * STATE : (hh + 1) * STATE]
                    )
        return carry

    def first_half():
        for cp in ups:
            cp.start(priority=1)
        prepare()
        lax.fori_loop(0, pairs // 2, update, 0)

    total = scatter(heads_out, outs, out_w, sums_a, land_a, send_a, recv_a, first_half)
    mine = (tokens[...].astype(jnp.float32) + total).astype(jnp.bfloat16)
    own_hidden[...] = mine
    for d in far_first(peers):
        send(own_hidden, hidden.at[d], send_h, recv_h, d)
    for d in order:
        downs[d].start(priority=1)
    lax.fori_loop(pairs // 2, pairs, update, 0)

    squares = jnp.zeros((rows, 1), jnp.float32)
    for d in range(peers):
        if d == 0:
            raw = mine
        else:
            arrived(own_hidden, hidden.at[d], send_h, recv_h, d)
            raw = hidden[d]
        x = raw.astype(jnp.float32)
        squares = squares + jnp.sum(x * x, axis=1, keepdims=True)
        scaled = jnp.concatenate(split(x * mlp_gain[:, pl.ds(place(d), part)]), axis=0)
        ups[d].wait()
        out = jnp.dot(scaled.astype(jnp.bfloat16), up_w[d], preferred_element_type=jnp.float32)
        out = out[:rows] + out[rows:]
        up = out if d == 0 else up + out

    inv = lax.rsqrt(squares / (peers * part) + NORM_EPS)
    up = jnp.maximum(up * inv, 0.0)
    squared[...] = (up * up).astype(jnp.bfloat16)
    total = scatter(
        squared[...], downs, down_w, sums_b, land_b, send_b, recv_b, lambda: None
    )
    layer_out[...] = (mine.astype(jnp.float32) + total).astype(jnp.bfloat16)
    for cp in pending:
        cp.wait_send()


def decode(peers, tokens, small, past_value, past_maps, weights, state, later):
    rows, part = tokens.shape
    heads = state.shape[1]
    inner, maps = heads * HEAD_DIM, 2 * heads * STATE
    hid = later[1].shape[1]
    width = 2 * inner
    chunks = 1 + maps // width
    f32, bf16 = jnp.float32, jnp.bfloat16
    block = 4 if rows % 4 == 0 else 2
    vmem = pl.BlockSpec(memory_space=pltpu.VMEM)
    hbm = pl.BlockSpec(memory_space=pl.ANY)
    sems = pltpu.SemaphoreType.DMA((peers,))
    slots = pltpu.VMEM((peers, rows, part), bf16)
    operands = (tokens, *small, past_value, past_maps, *weights, state, *later)
    return pl.pallas_call(
        functools.partial(decode_kernel, peers),
        out_shape=(
            pltpu.VMEM((rows, part), bf16),
            pltpu.VMEM((rows, inner), bf16),
            pltpu.VMEM((rows, maps), bf16),
            pltpu.VMEM(past_value.shape, bf16),
            pltpu.VMEM(past_maps.shape, bf16),
            pltpu.VMEM(state.shape, f32),
        ),
        in_specs=[hbm] * len(operands),
        out_specs=(vmem,) * 6,
        scratch_shapes=[
            pltpu.VMEM((rows, part), bf16),
            *[pltpu.VMEM(x.shape, x.dtype) for x in small],
            slots,
            pltpu.VMEM((peers, chunks, part, width), bf16),
            pltpu.VMEM((chunks, rows, width), f32),
            pltpu.VMEM((rows, inner), f32),
            pltpu.VMEM((rows, inner), f32),
            pltpu.VMEM((rows, maps), bf16),
            pltpu.VMEM((heads, rows, STATE), f32),
            pltpu.VMEM((rows, inner), f32),
            pltpu.VMEM((heads // 2, HEAD_DIM, STATE), bf16),
            pltpu.VMEM((rows, 16, STATE), bf16),
            pltpu.VMEM((heads // 2, 2 * rows, STATE), bf16),
            pltpu.VMEM((heads // 2, 2 * rows, STATE), f32),
            pltpu.VMEM((peers, inner, part), bf16),
            pltpu.VMEM((peers, part, hid), bf16),
            pltpu.VMEM((peers, hid, part), bf16),
            slots,
            slots,
            pltpu.VMEM((rows, part), bf16),
            slots,
            pltpu.VMEM((rows, hid), bf16),
            slots,
            slots,
            pltpu.SemaphoreType.DMA((12,)),
            pltpu.SemaphoreType.DMA((peers, chunks)),
            pltpu.SemaphoreType.DMA((rows // block,)),
            *[sems] * 11,
        ],
        compiler_params=pltpu.CompilerParams(
            collective_id=0, has_side_effects=True, vmem_limit_bytes=FUSED_LIMIT
        ),
        name="decode",
    )(*in_hbm(*operands))


def flush_kernel(
    layer,
    value_new,
    maps_new,
    past_value,
    past_maps,
    state,
    layer_out,
    state_out,
    value_tail,
    maps_tail,
    sem,
    state_sem,
):
    taps = past_value.shape[0]
    blocks = state_sem.shape[0]
    block = state.shape[0] // blocks
    copies = []
    for k in range(blocks):
        at = pl.ds(k * block, block)
        copies.append(pltpu.make_async_copy(state.at[at], state_out.at[at], state_sem.at[k]))
    for k, (past, new, tail) in enumerate(
        ((past_value, value_new, value_tail), (past_maps, maps_new, maps_tail))
    ):
        keep = past.at[pl.ds(1, taps - 1)]
        copies.append(
            pltpu.make_async_copy(keep, tail.at[pl.ds(0, taps - 1)], sem.at[2 * k])
        )
        copies.append(pltpu.make_async_copy(new, tail.at[taps - 1], sem.at[2 * k + 1]))
    copies.append(pltpu.make_async_copy(layer, layer_out, sem.at[4]))
    for cp in copies:
        cp.start(priority=1)
    for cp in copies:
        cp.wait()


def flush(parts):
    layer, _, _, past_v, past_m, state = parts
    f32, bf16 = jnp.float32, jnp.bfloat16
    vmem = pl.BlockSpec(memory_space=pltpu.VMEM)
    hbm = pl.BlockSpec(memory_space=pl.ANY)
    rows = state.shape[0]
    return pl.pallas_call(
        flush_kernel,
        out_shape=(
            pltpu.HBM(layer.shape, bf16),
            pltpu.HBM(state.shape, f32),
            pltpu.HBM(past_v.shape, bf16),
            pltpu.HBM(past_m.shape, bf16),
        ),
        in_specs=[vmem] * 6,
        out_specs=(hbm,) * 4,
        scratch_shapes=[
            pltpu.SemaphoreType.DMA((5,)),
            pltpu.SemaphoreType.DMA((8 if rows % 8 == 0 else 1,)),
        ],
        compiler_params=pltpu.CompilerParams(vmem_limit_bytes=4 * 1024 * 1024),
        name="flush",
    )(*in_vmem(*parts))


def local_kernels(
    peers,
    tokens,
    mix_gain,
    w_gate,
    w_value,
    w_maps,
    w_step,
    conv_value,
    conv_maps,
    past_value,
    past_maps,
    step_bias,
    decay_log,
    skip_gain,
    head_gain,
    state,
    w_out,
    mlp_gain,
    w_up,
    w_down,
):
    small = (
        mix_gain[None, :],
        w_step.T,
        step_bias[None, :],
        decay_log[None, :],
        skip_gain[None, :],
        head_gain[None, :],
        mlp_gain[None, :],
        conv_value,
        conv_maps,
    )
    parts = decode(
        peers,
        tokens,
        small,
        jnp.swapaxes(past_value, 0, 1),
        jnp.swapaxes(past_maps, 0, 1),
        (w_gate, w_value, w_maps),
        state,
        (w_out, w_up, w_down),
    )
    layer_out, state_next, tail_v, tail_m = flush(parts)
    return layer_out, state_next, jnp.swapaxes(tail_v, 0, 1), jnp.swapaxes(tail_m, 0, 1)


def kernels_fit(peers, tokens, state, w_maps, w_up):
    rows, part = tokens.shape
    heads = state.shape[1]
    inner = heads * HEAD_DIM
    weights = 2 * tokens.shape[1] * peers * (2 * inner + w_maps.shape[1])
    later = 2 * part * peers * (inner + 2 * w_up.shape[1])
    held = 4 * rows * heads * HEAD_DIM * STATE
    return (
        peers > 1
        and peers & (peers - 1) == 0
        and rows % 8 == 0
        and 4 * rows <= STATE
        and part % 128 == 0
        and heads % 4 == 0
        and w_maps.shape[1] == heads * 2 * STATE
        and w_up.shape[1] % 128 == 0
        and weights + later <= 44 * 1024 * 1024
        and held <= 12 * 1024 * 1024
    )


def rms_rows(matrix, gain_vec):
    widened = matrix.astype(jnp.float32)
    inv_scale = lax.rsqrt(jnp.mean(widened * widened, axis=-1, keepdims=True) + NORM_EPS)
    return (widened * inv_scale * gain_vec).astype(jnp.bfloat16)


def short_conv(past_rows, newest, kernel):
    window = jnp.concatenate([past_rows, newest[:, None, :]], axis=1)
    summed = jnp.sum(window.astype(jnp.float32) * kernel[None], axis=1)
    return (jax.nn.silu(summed), window[:, 1:, :])


def local(
    tokens,
    mix_gain,
    w_gate,
    w_value,
    w_maps,
    w_step,
    conv_value,
    conv_maps,
    past_value,
    past_maps,
    step_bias,
    decay_log,
    skip_gain,
    head_gain,
    state,
    w_out,
    mlp_gain,
    w_up,
    w_down,
):
    whole_rows = lax.all_gather(tokens, "kv", axis=1, tiled=True)
    batch_rows = whole_rows.shape[0]
    heads_here = state.shape[1]
    head_start = lax.axis_index("kv") * heads_here
    normed = rms_rows(whole_rows, mix_gain)
    gate_pre = jnp.dot(normed, w_gate, preferred_element_type=jnp.float32)
    step_cols = lax.dynamic_slice_in_dim(w_step, head_start, heads_here, 1)
    step_pre = jnp.dot(normed, step_cols, preferred_element_type=jnp.float32)
    value_new = jnp.dot(normed, w_value, preferred_element_type=jnp.float32).astype(jnp.bfloat16)
    maps_new = jnp.dot(normed, w_maps, preferred_element_type=jnp.float32).astype(jnp.bfloat16)
    value_act, value_tail = short_conv(past_value, value_new, conv_value)
    maps_act, maps_tail = short_conv(past_maps, maps_new, conv_maps)
    maps_act = lax.optimization_barrier(maps_act.astype(jnp.bfloat16))
    grouped = maps_act.astype(jnp.float32).reshape(batch_rows, -1, 2, STATE)
    per_group = heads_here // grouped.shape[1]
    in_map = jnp.repeat(grouped[:, :, 0], per_group, axis=1)
    out_map = jnp.repeat(grouped[:, :, 1], per_group, axis=1)
    head_values = value_act.reshape(batch_rows, heads_here, HEAD_DIM)
    step_size = jax.nn.softplus(step_pre + step_bias)
    decay_rate = jnp.exp(-step_size * jnp.exp(decay_log))
    written = (step_size[:, :, None] * head_values)[:, :, :, None] * in_map[:, :, None, :]
    state_next = decay_rate[:, :, None, None] * state + written
    read_out = (
        jnp.sum(state_next * out_map[:, :, None, :], axis=-1)
        + skip_gain[None, :, None] * head_values
    )
    gated_heads = read_out * jax.nn.silu(gate_pre.reshape(batch_rows, heads_here, HEAD_DIM))
    inv_scale = lax.rsqrt(jnp.mean(gated_heads * gated_heads, axis=-1, keepdims=True) + NORM_EPS)
    heads_out = gated_heads * inv_scale * head_gain.reshape(heads_here, HEAD_DIM)
    heads_out = heads_out.reshape(batch_rows, heads_here * HEAD_DIM).astype(jnp.bfloat16)
    partial_value = jnp.dot(heads_out, w_out, preferred_element_type=jnp.float32)
    own_part = lax.psum_scatter(partial_value, "kv", scatter_dimension=1, tiled=True)
    own_hidden = lax.optimization_barrier(
        (tokens.astype(jnp.float32) + own_part).astype(jnp.bfloat16)
    )
    hidden = lax.all_gather(own_hidden, "kv", axis=1, tiled=True)
    normed_mlp = rms_rows(hidden, mlp_gain)
    squared = jnp.square(jax.nn.relu(jnp.dot(normed_mlp, w_up, preferred_element_type=jnp.float32)))
    squared = squared.astype(jnp.bfloat16)
    partial_mlp = jnp.dot(squared, w_down, preferred_element_type=jnp.float32)
    mlp_part = lax.psum_scatter(partial_mlp, "kv", scatter_dimension=1, tiled=True)
    layer_out = (own_hidden.astype(jnp.float32) + mlp_part).astype(jnp.bfloat16)
    return (layer_out, state_next, value_tail, maps_tail)


def solution(mesh):
    in_specs = (
        P(("dp", "tp"), "kv"),
        P(),
        P(None, "kv"),
        P(None, "kv"),
        P(None, "kv"),
        P(),
        P(None, "kv"),
        P(None, "kv"),
        P(("dp", "tp"), None, "kv"),
        P(("dp", "tp"), None, "kv"),
        P("kv"),
        P("kv"),
        P("kv"),
        P("kv"),
        P(("dp", "tp"), "kv", None, None),
        P("kv", None),
        P(),
        P(None, "kv"),
        P("kv", None),
    )
    out_specs = (
        P(("dp", "tp"), "kv"),
        P(("dp", "tp"), "kv", None, None),
        P(("dp", "tp"), None, "kv"),
        P(("dp", "tp"), None, "kv"),
    )
    peers = mesh.shape["kv"]

    def device_part(*args):
        if kernels_fit(peers, args[0], args[14], args[4], args[17]):
            return local_kernels(peers, *args)
        return local(*args)

    return jax.shard_map(
        device_part, mesh=mesh, in_specs=in_specs, out_specs=out_specs, check_vma=False
    )
```

```python
import functools

import jax
import jax.numpy as jnp
from jax import lax
from jax.experimental import pallas as pl
from jax.experimental.pallas import tpu as pltpu
from jax.sharding import PartitionSpec as P

HEAD_DIM = 64
STATE = 128
MESH = pl.DeviceIdType.MESH
FUSED_LIMIT = 49 * 1024 * 1024
WINDOW = 9
SIDES = 2


NORM_EPS = 1e-05
NT = (((1,), (1,)), ((), ()))


def partner(me, d):
    other = me
    bit = 1
    while bit <= d:
        if d & bit:
            other = other + bit - 2 * bit * lax.rem(lax.div(me, bit), 2)
        bit *= 2
    return other


def greet(peers, me, side):
    for d in range(peers):
        for t in range(SIDES):
            if d > 0 or t > 0:
                pl.semaphore_signal(
                    pltpu.get_barrier_semaphore(),
                    inc=1,
                    device_id={"kv": partner(me, d), "tp": lax.rem(side + t, SIDES)},
                    device_id_type=MESH,
                )


def all_here(peers):
    pl.semaphore_wait(pltpu.get_barrier_semaphore(), SIDES * peers - 1)


def far_first(peers):
    return list(range(1, peers))[::-1]


def push(src, dst, send_sem, recv_sem, target):
    return pltpu.make_async_remote_copy(
        src_ref=src,
        dst_ref=dst,
        send_sem=send_sem,
        recv_sem=recv_sem,
        device_id=target,
        device_id_type=MESH,
    )


def in_hbm(*arrays):
    return [pltpu.with_memory_space_constraint(x, pltpu.HBM) for x in arrays]


def in_vmem(*arrays):
    return [pltpu.with_memory_space_constraint(x, pltpu.VMEM) for x in arrays]


def silu(x):
    return x * jax.nn.sigmoid(x)


def split(x):
    high = x.astype(jnp.bfloat16).astype(jnp.float32)
    return high, x - high


def decode_kernel(
    peers,
    tokens_in,
    gain_in,
    w_step_in,
    bias_in,
    decay_log_in,
    skip_in,
    head_gain_in,
    mlp_gain_in,
    conv_value_in,
    conv_maps_in,
    past_value_in,
    past_maps_in,
    w_gate,
    w_value,
    w_maps,
    state_in,
    w_out,
    w_up,
    w_down,
    layer_out,
    value_new,
    maps_new,
    past_value,
    past_maps,
    state,
    tokens,
    gain,
    w_step,
    bias,
    decay_log,
    skip,
    head_gain,
    mlp_gain,
    conv_value,
    conv_maps,
    slots,
    twin,
    give_gate,
    give_value,
    give_maps,
    land_gate,
    land_value,
    land_maps,
    weights,
    acc,
    gate,
    value_act,
    maps_act,
    decay_rows,
    step_cols,
    skip_cols,
    spread,
    pick,
    readers,
    direct,
    read,
    heads_out,
    out_w,
    up_w,
    down_w,
    sums_a,
    land_a,
    own_hidden,
    hidden,
    squared,
    sums_b,
    land_b,
    small_sem,
    w_sem,
    state_sem,
    out_sem,
    up_sem,
    down_sem,
    send_t,
    recv_t,
    send_a,
    recv_a,
    send_h,
    recv_h,
    send_b,
    recv_b,
    send_f,
    recv_f,
    send_x,
    recv_x,
):
    me = lax.axis_index("kv")
    rows, part = tokens.shape
    chunks, width = weights.shape[1], weights.shape[3]
    heads = bias.shape[1]
    inner = value_new.shape[1]
    pair = 2 * HEAD_DIM
    wide = 4 * STATE
    taps = past_value.shape[0]
    pairs = heads // 2
    side = lax.axis_index("tp")
    greet(peers, me, side)

    def place(d):
        return pl.multiple_of(partner(me, d) * part, part)

    small = [
        pltpu.make_async_copy(src, dst, small_sem.at[k])
        for k, (src, dst) in enumerate(
            (
                (tokens_in, tokens),
                (gain_in, gain),
                (w_step_in, w_step),
                (bias_in, bias),
                (decay_log_in, decay_log),
                (skip_in, skip),
                (head_gain_in, head_gain),
                (mlp_gain_in, mlp_gain),
                (conv_value_in, conv_value),
                (conv_maps_in, conv_maps),
                (past_value_in, past_value),
                (past_maps_in, past_maps),
            )
        )
    ]

    half = inner // 2
    half_at = pl.ds(pl.multiple_of(side * half, half), half)

    def maps_at(t, c):
        return pl.ds(pl.multiple_of(t * 2 * width + (c - 1) * width, width), width)

    def weight_copies(d, c):
        if c == 0:
            return [
                pltpu.make_async_copy(
                    ref.at[pl.ds(place(d), part), half_at],
                    weights.at[d, 0, :, pl.ds(k * half, half)],
                    w_sem.at[d, 0],
                )
                for k, ref in enumerate((w_gate, w_value))
            ]
        return [
            pltpu.make_async_copy(
                w_maps.at[pl.ds(place(d), part), maps_at(side, c)], weights.at[d, c], w_sem.at[d, c]
            )
        ]

    blocks = state_sem.shape[0]
    block = rows // blocks

    def state_copy(r):
        at = pl.ds(r * block, block)
        return pltpu.make_async_copy(state_in.at[at], state.at[at], state_sem.at[r])

    order = far_first(peers) + [0]
    outs = [
        pltpu.make_async_copy(w_out.at[:, pl.ds(place(d), part)], out_w.at[d], out_sem.at[d])
        for d in range(peers)
    ]
    ups = [
        pltpu.make_async_copy(w_up.at[pl.ds(place(d), part), :], up_w.at[d], up_sem.at[d])
        for d in range(peers)
    ]
    downs = [
        pltpu.make_async_copy(w_down.at[:, pl.ds(place(d), part)], down_w.at[d], down_sem.at[d])
        for d in range(peers)
    ]
    bulk = [weight_copies(d, c) for d in range(peers) for c in range(chunks)]
    bulk += [[state_copy(r)] for r in range(blocks)] + [[outs[d]] for d in order]

    def load(count):
        for _ in range(min(count, len(bulk))):
            for cp in bulk.pop(0):
                cp.start(priority=1)

    for cp in small[:3]:
        cp.start()
    load(chunks)
    small[0].wait()
    all_here(peers)
    pending = []

    def send(src, dst, send_sem, recv_sem, d, t):
        cp = push(src, dst, send_sem, recv_sem, {"kv": partner(me, d), "tp": t})
        cp.start()
        return cp

    def arrived(dst, recv_sem):
        push(dst, dst, recv_sem, recv_sem, {"kv": me, "tp": side}).wait_recv()

    for d in far_first(peers):
        pending.append(send(tokens, slots.at[d], send_t.at[d], recv_t.at[d], d, side))

    facing = lax.rem(side + 1, SIDES)
    pending.append(send(tokens, twin.at[0], send_f.at[0], recv_f.at[0], 0, facing))
    for cp in small[3:]:
        cp.start()
    load(WINDOW - chunks)
    for cp in small[1:]:
        cp.wait()

    lane = lax.broadcasted_iota(jnp.int32, (rows, pair), 1)

    def by_head(table, h):
        return jnp.where(lane < HEAD_DIM, table[:, h : h + 1], table[:, h + 1 : h + 2])

    both = SIDES * rows
    squares = jnp.zeros((both, 1), jnp.float32)
    step_pre = jnp.zeros((2 * both, w_step.shape[0]), jnp.float32)
    for d in range(peers):
        if d == 0:
            ahead = [1] if peers > 1 else []
        else:
            ahead = [d + 1] if d + 1 < peers else []
        arrived(twin.at[d], recv_f.at[d])
        raw = [tokens[...] if d == 0 else slots[d], twin[d]]
        x = jnp.concatenate([half_rows.astype(jnp.float32) for half_rows in raw], axis=0)
        squares = squares + jnp.sum(x * x, axis=1, keepdims=True)
        scaled = jnp.concatenate(split(x * gain[:, pl.ds(place(d), part)]), axis=0)
        scaled = scaled.astype(jnp.bfloat16)
        step_pre = step_pre + lax.dot_general(
            scaled, w_step[:, pl.ds(place(d), part)], NT, preferred_element_type=jnp.float32
        )
        for e in ahead:
            arrived(slots.at[e], recv_t.at[e])
            pending.append(send(slots.at[e], twin.at[e], send_f.at[e], recv_f.at[e], 0, facing))
        last = d == peers - 1
        if last:
            inv = lax.rsqrt(squares / (peers * part) + NORM_EPS)
        for c in range(chunks):
            pltpu.make_async_copy(
                w_maps.at[pl.ds(0, part), pl.ds(0, width)], weights.at[d, c], w_sem.at[d, c]
            ).wait()
            load(1)
            out = jnp.dot(scaled, weights[d, c], preferred_element_type=jnp.float32)
            out = out[:both] + out[both:]
            total = out if d == 0 else acc[c] + out
            if not last:
                acc[c] = total
                continue
            total = total * inv
            if c == 0:
                gate[:, half_at] = total[:rows, :half]
                value_new[:, half_at] = total[:rows, half:].astype(jnp.bfloat16)
                give_gate[...] = total[rows:, :half]
                give_value[...] = total[rows:, half:].astype(jnp.bfloat16)
                pending.append(send(give_gate, land_gate, send_x.at[c], recv_x.at[c], 0, facing))
                pending.append(
                    send(
                        give_value, land_value, send_x.at[chunks], recv_x.at[chunks], 0, facing
                    )
                )
            else:
                maps_new[:, maps_at(side, c)] = total[:rows].astype(jnp.bfloat16)
                give_maps[c] = total[rows:].astype(jnp.bfloat16)
                pending.append(
                    send(give_maps.at[c], land_maps.at[c], send_x.at[c], recv_x.at[c], 0, facing)
                )

    step_pre = (step_pre[:rows] + step_pre[both : both + rows]) * inv[:rows]
    own = step_pre[:, :heads]
    for j in range(1, peers):
        own = jnp.where(me == j, step_pre[:, j * heads : (j + 1) * heads], own)
    own = own + bias[...]
    step = jnp.maximum(own, 0.0) + jnp.log1p(jnp.exp(-jnp.abs(own)))
    decay = jnp.exp(-step * jnp.exp(decay_log[...]))
    for h in range(heads):
        decay_rows[h] = jnp.broadcast_to(decay[:, h : h + 1], (rows, STATE))
    for h in range(0, heads, 2):
        step_cols[:, h * HEAD_DIM : (h + 2) * HEAD_DIM] = by_head(step, h)

    for h in range(0, heads, 2):
        skip_cols[:, h * HEAD_DIM : (h + 2) * HEAD_DIM] = by_head(skip, h)

    def conv(fresh, past, cols, table):
        summed = fresh[:, cols].astype(jnp.float32) * table[taps : taps + 1, cols]
        for k in range(taps):
            old = past[k, :, cols].astype(jnp.float32)
            summed = summed + old * table[k : k + 1, cols]
        return silu(summed)

    row = lax.broadcasted_iota(jnp.int32, (2 * rows, STATE), 0)
    column = lax.broadcasted_iota(jnp.int32, (2 * rows, STATE), 1)
    seq = jnp.where(row >= rows, row - rows, row)
    owner = jnp.where((row >= rows) == (column >= HEAD_DIM), seq, -1)
    read[...] = jnp.zeros_like(read)
    early = lax.rem(seq, 4) < 2
    first = lane < HEAD_DIM

    def ready(t):
        cols = pl.ds(pl.multiple_of(t * half, half), half)
        gate[:, cols] = silu(gate[:, cols])
        value_act[:, cols] = conv(value_new, past_value, cols, conv_value)
        for c in range(1, chunks):
            cols = maps_at(t, c)
            maps_act[:, cols] = conv(maps_new, past_maps, cols, conv_maps).astype(jnp.bfloat16)
        for k in range(pairs // 2):
            i = t * (pairs // 2) + k
            maps = maps_act[:, pl.ds(pl.multiple_of(i * wide, wide), wide)].astype(jnp.float32)
            outof = [maps[:, m * STATE : (m + 1) * STATE] for m in range(4)]
            stacked = jnp.concatenate([outof[1], outof[3]], axis=0)
            readers[i] = jnp.concatenate(
                [jnp.where(early, stacked, 0.0), jnp.where(early, 0.0, stacked)], axis=1
            ).astype(jnp.bfloat16)
            at = pl.ds(pl.multiple_of(i * pair, pair), pair)
            act = value_act[:, at]
            dots = [jnp.sum(outof[m] * outof[m + 1], axis=1, keepdims=True) for m in (0, 2)]
            dots = jnp.where(first, dots[0], dots[1])
            direct[:, at] = dots * (act * step_cols[:, at]) + skip_cols[:, at] * act

    def read_pair(i, r):
        strips = []
        for k in range(2):
            for hh in range(2):
                h = 2 * i + hh
                strips.append(
                    jnp.concatenate(
                        [state[r * block + k, h], state[r * block + k + 2, h]], axis=1
                    ).astype(jnp.bfloat16)
                )
        found = lax.dot_general(
            readers[i], jnp.concatenate(strips, axis=0), NT, preferred_element_type=jnp.float32
        )
        total = read[i]
        for k in range(2):
            hit = (owner == r * block + k) | (owner == r * block + k + 2)
            total = total + jnp.where(hit, found[:, k * pair : (k + 1) * pair], 0.0)
        read[i] = total

    ready(side)
    for r in range(blocks):
        state_copy(r).wait()
        load(1)
        for k in range(pairs // 2):
            read_pair(side * (pairs // 2) + k, r)
    load(len(bulk))
    facing_half = pl.ds(pl.multiple_of(facing * half, half), half)
    arrived(land_gate, recv_x.at[0])
    gate[:, facing_half] = land_gate[...]
    arrived(land_value, recv_x.at[chunks])
    value_new[:, facing_half] = land_value[...]
    for c in range(1, chunks):
        arrived(land_maps.at[c], recv_x.at[c])
        maps_new[:, maps_at(facing, c)] = land_maps[c]
    ready(facing)
    for r in range(blocks):
        for k in range(pairs // 2):
            read_pair(facing * (pairs // 2) + k, r)

    for i in range(pairs):
        at = slice(i * pair, (i + 1) * pair)
        h = 2 * i
        decayed = jnp.where(first, decay_rows[h], decay_rows[h + 1])
        found = read[i]
        gated = (decayed * (found[:rows] + found[rows:]) + direct[:, at]) * gate[:, at]
        square = gated * gated
        low = jnp.sum(jnp.where(first, square, 0.0), axis=1, keepdims=True)
        top = jnp.sum(jnp.where(first, 0.0, square), axis=1, keepdims=True)
        norm = lax.rsqrt(jnp.where(first, low, top) / HEAD_DIM + NORM_EPS)
        heads_out[:, at] = (gated * norm * head_gain[:, at]).astype(jnp.bfloat16)

    def prepare():
        spot = lax.broadcasted_iota(jnp.int32, (16, STATE), 1)
        for b in range(rows):
            hit = (spot == b) | (spot == rows + b)
            hit = hit | (spot == 2 * rows + b) | (spot == 3 * rows + b)
            pick[b] = jnp.where(hit, 1.0, 0.0).astype(jnp.bfloat16)
        blank = jnp.zeros((STATE - 4 * rows, HEAD_DIM), jnp.float32)
        for i in range(pairs):
            at = slice(i * pair, (i + 1) * pair)
            both = jnp.concatenate(split(value_act[:, at] * step_cols[:, at]), axis=0)
            stack = jnp.concatenate([both[:, :HEAD_DIM], both[:, HEAD_DIM:], blank], axis=0)
            spread[i] = stack.T.astype(jnp.bfloat16)

    def update(i, carry):
        maps = maps_act[:, pl.ds(pl.multiple_of(i * wide, wide), wide)].astype(jnp.float32)
        ins = []
        for hh in range(2):
            ins += [maps[:, 2 * hh * STATE : (2 * hh + 1) * STATE]] * 2
        blank = jnp.zeros((2 * rows, STATE), jnp.float32)
        none = jnp.zeros((STATE - 4 * rows, STATE), jnp.float32)
        left = jnp.concatenate(ins[:2] + [blank, none], axis=0)
        right = jnp.concatenate([blank] + ins[2:] + [none], axis=0)
        into = jnp.concatenate([left, right], axis=1).astype(jnp.bfloat16)
        values = spread[i]
        for b in range(0, rows, 4):
            chosen = jnp.concatenate(
                [
                    values * jnp.concatenate([pick[b + k]] * (HEAD_DIM // 16), axis=0)
                    for k in range(4)
                ],
                axis=0,
            )
            written = jnp.dot(chosen, into, preferred_element_type=jnp.float32)
            for k in range(4):
                for hh in range(2):
                    h = 2 * i + hh
                    state[b + k, h] = (
                        decay_rows[h, pl.ds(b + k, 1), :] * state[b + k, h]
                        + written[k * HEAD_DIM : (k + 1) * HEAD_DIM, hh * STATE : (hh + 1) * STATE]
                    )
        return carry

    def out_piece(d):
        outs[d].wait()
        return jnp.dot(heads_out[...], out_w[d], preferred_element_type=jnp.float32)

    def give_sums(t, targets):
        sent = []
        for d in targets:
            sums_a[d] = out_piece(d).astype(jnp.bfloat16)
            sent.append(
                send(sums_a.at[d], land_a.at[t, d], send_a.at[d], recv_a.at[t, d], d, 1)
            )
        return sent

    @pl.when(side == 0)
    def _():
        sent = give_sums(0, order)
        prepare()
        lax.fori_loop(0, pairs, update, 0)
        arrived(own_hidden.at[0], recv_h.at[0])
        total = own_hidden[0].astype(jnp.float32)
        for d in range(peers):
            arrived(land_b.at[d], recv_b.at[d])
            total = total + land_b[d].astype(jnp.float32)
        layer_out[...] = total.astype(jnp.bfloat16)
        for cp in sent:
            cp.wait_send()

    @pl.when(side == 1)
    def _():
        sent = give_sums(1, far_first(peers))
        mine = tokens[...].astype(jnp.float32) + out_piece(0)
        for cp in ups:
            cp.start(priority=1)
        prepare()
        lax.fori_loop(0, pairs // 2, update, 0)
        other = twin[0].astype(jnp.float32)
        for d in range(peers):
            if d > 0:
                arrived(land_a.at[1, d], recv_a.at[1, d])
                mine = mine + land_a[1, d].astype(jnp.float32)
            arrived(land_a.at[0, d], recv_a.at[0, d])
            other = other + land_a[0, d].astype(jnp.float32)
        own_hidden[0] = other.astype(jnp.bfloat16)
        own_hidden[1] = mine.astype(jnp.bfloat16)
        for d in far_first(peers):
            sent.append(send(own_hidden, hidden.at[d], send_h.at[d], recv_h.at[d], d, 1))
        sent.append(
            send(own_hidden.at[0], own_hidden.at[0], send_h.at[0], recv_h.at[0], 0, 0)
        )
        for d in order:
            downs[d].start(priority=1)
        lax.fori_loop(pairs // 2, pairs, update, 0)

        squares = jnp.zeros((both, 1), jnp.float32)
        for d in range(peers):
            if d == 0:
                raw = [own_hidden[t] for t in range(SIDES)]
            else:
                arrived(hidden.at[d], recv_h.at[d])
                raw = [hidden[d, t] for t in range(SIDES)]
            x = jnp.concatenate([part_t.astype(jnp.float32) for part_t in raw], axis=0)
            squares = squares + jnp.sum(x * x, axis=1, keepdims=True)
            scaled = jnp.concatenate(split(x * mlp_gain[:, pl.ds(place(d), part)]), axis=0)
            ups[d].wait()
            out = jnp.dot(scaled.astype(jnp.bfloat16), up_w[d], preferred_element_type=jnp.float32)
            out = out[:both] + out[both:]
            up = out if d == 0 else up + out

        inv = lax.rsqrt(squares / (peers * part) + NORM_EPS)
        up = jnp.maximum(up * inv, 0.0)
        squared[...] = (up * up).astype(jnp.bfloat16)
        for d in order:
            downs[d].wait()
            piece = jnp.dot(squared[...], down_w[d], preferred_element_type=jnp.float32)
            sums_b[0, d] = piece[:rows].astype(jnp.bfloat16)
            sent.append(
                send(sums_b.at[0, d], land_b.at[d], send_b.at[0, d], recv_b.at[d], d, 0)
            )
            if d > 0:
                sums_b[1, d] = piece[rows:].astype(jnp.bfloat16)
                sent.append(
                    send(sums_b.at[1, d], land_b.at[d], send_b.at[1, d], recv_b.at[d], d, 1)
                )
            else:
                total = own_hidden[1].astype(jnp.float32) + piece[rows:]
        for d in range(1, peers):
            arrived(land_b.at[d], recv_b.at[d])
            total = total + land_b[d].astype(jnp.float32)
        layer_out[...] = total.astype(jnp.bfloat16)
        for cp in sent:
            cp.wait_send()

    for cp in pending:
        cp.wait_send()


def decode(peers, tokens, small, past_value, past_maps, weights, state, later):
    rows, part = tokens.shape
    heads = state.shape[1]
    inner, maps = heads * HEAD_DIM, 2 * heads * STATE
    hid = later[1].shape[1]
    width = inner
    chunks = 1 + maps // (2 * width)
    f32, bf16 = jnp.float32, jnp.bfloat16
    block = 4
    vmem = pl.BlockSpec(memory_space=pltpu.VMEM)
    hbm = pl.BlockSpec(memory_space=pl.ANY)
    sems = pltpu.SemaphoreType.DMA((peers,))
    slots = pltpu.VMEM((peers, rows, part), bf16)
    both_slots = pltpu.VMEM((SIDES, peers, rows, part), bf16)
    both_sems = pltpu.SemaphoreType.DMA((SIDES, peers))
    operands = (tokens, *small, past_value, past_maps, *weights, state, *later)
    return pl.pallas_call(
        functools.partial(decode_kernel, peers),
        out_shape=(
            pltpu.VMEM((rows, part), bf16),
            pltpu.VMEM((rows, inner), bf16),
            pltpu.VMEM((rows, maps), bf16),
            pltpu.VMEM(past_value.shape, bf16),
            pltpu.VMEM(past_maps.shape, bf16),
            pltpu.VMEM(state.shape, f32),
        ),
        in_specs=[hbm] * len(operands),
        out_specs=(vmem,) * 6,
        scratch_shapes=[
            pltpu.VMEM((rows, part), bf16),
            *[pltpu.VMEM(x.shape, x.dtype) for x in small],
            slots,
            slots,
            pltpu.VMEM((rows, inner // 2), f32),
            pltpu.VMEM((rows, inner // 2), bf16),
            pltpu.VMEM((chunks, rows, width), bf16),
            pltpu.VMEM((rows, inner // 2), f32),
            pltpu.VMEM((rows, inner // 2), bf16),
            pltpu.VMEM((chunks, rows, width), bf16),
            pltpu.VMEM((peers, chunks, part, width), bf16),
            pltpu.VMEM((chunks, SIDES * rows, width), f32),
            pltpu.VMEM((rows, inner), f32),
            pltpu.VMEM((rows, inner), f32),
            pltpu.VMEM((rows, maps), bf16),
            pltpu.VMEM((heads, rows, STATE), f32),
            pltpu.VMEM((rows, inner), f32),
            pltpu.VMEM((rows, inner), f32),
            pltpu.VMEM((heads // 2, HEAD_DIM, STATE), bf16),
            pltpu.VMEM((rows, 16, STATE), bf16),
            pltpu.VMEM((heads // 2, 2 * rows, 2 * STATE), bf16),
            pltpu.VMEM((rows, inner), f32),
            pltpu.VMEM((heads // 2, 2 * rows, STATE), f32),
            pltpu.VMEM((rows, inner), bf16),
            pltpu.VMEM((peers, inner, part), bf16),
            pltpu.VMEM((peers, part, hid), bf16),
            pltpu.VMEM((peers, hid, part), bf16),
            slots,
            both_slots,
            pltpu.VMEM((SIDES, rows, part), bf16),
            pltpu.VMEM((peers, SIDES, rows, part), bf16),
            pltpu.VMEM((SIDES * rows, hid), bf16),
            both_slots,
            slots,
            pltpu.SemaphoreType.DMA((12,)),
            pltpu.SemaphoreType.DMA((peers, chunks)),
            pltpu.SemaphoreType.DMA((rows // block,)),
            sems,
            sems,
            sems,
            sems,
            sems,
            sems,
            both_sems,
            sems,
            sems,
            both_sems,
            sems,
            sems,
            sems,
            pltpu.SemaphoreType.DMA((chunks + 1,)),
            pltpu.SemaphoreType.DMA((chunks + 1,)),
        ],
        compiler_params=pltpu.CompilerParams(
            collective_id=0, has_side_effects=True, vmem_limit_bytes=FUSED_LIMIT
        ),
        name="decode",
    )(*in_hbm(*operands))


def flush_kernel(
    layer,
    value_new,
    maps_new,
    past_value,
    past_maps,
    state,
    layer_out,
    state_out,
    value_tail,
    maps_tail,
    sem,
    state_sem,
):
    taps = past_value.shape[0]
    blocks = state_sem.shape[0]
    block = state.shape[0] // blocks
    copies = []
    for k in range(blocks):
        at = pl.ds(k * block, block)
        copies.append(pltpu.make_async_copy(state.at[at], state_out.at[at], state_sem.at[k]))
    for k, (past, new, tail) in enumerate(
        ((past_value, value_new, value_tail), (past_maps, maps_new, maps_tail))
    ):
        keep = past.at[pl.ds(1, taps - 1)]
        copies.append(
            pltpu.make_async_copy(keep, tail.at[pl.ds(0, taps - 1)], sem.at[2 * k])
        )
        copies.append(pltpu.make_async_copy(new, tail.at[taps - 1], sem.at[2 * k + 1]))
    copies.append(pltpu.make_async_copy(layer, layer_out, sem.at[4]))
    for cp in copies:
        cp.start(priority=1)
    for cp in copies:
        cp.wait()


def flush(parts):
    layer, _, _, past_v, past_m, state = parts
    f32, bf16 = jnp.float32, jnp.bfloat16
    vmem = pl.BlockSpec(memory_space=pltpu.VMEM)
    hbm = pl.BlockSpec(memory_space=pl.ANY)
    rows = state.shape[0]
    return pl.pallas_call(
        flush_kernel,
        out_shape=(
            pltpu.HBM(layer.shape, bf16),
            pltpu.HBM(state.shape, f32),
            pltpu.HBM(past_v.shape, bf16),
            pltpu.HBM(past_m.shape, bf16),
        ),
        in_specs=[vmem] * 6,
        out_specs=(hbm,) * 4,
        scratch_shapes=[
            pltpu.SemaphoreType.DMA((5,)),
            pltpu.SemaphoreType.DMA((8 if rows % 8 == 0 else 1,)),
        ],
        compiler_params=pltpu.CompilerParams(vmem_limit_bytes=4 * 1024 * 1024),
        name="flush",
    )(*in_vmem(*parts))


def local_kernels(
    peers,
    tokens,
    mix_gain,
    w_gate,
    w_value,
    w_maps,
    w_step,
    conv_value,
    conv_maps,
    past_value,
    past_maps,
    step_bias,
    decay_log,
    skip_gain,
    head_gain,
    state,
    w_out,
    mlp_gain,
    w_up,
    w_down,
):
    small = (
        mix_gain[None, :],
        w_step.T,
        step_bias[None, :],
        decay_log[None, :],
        skip_gain[None, :],
        head_gain[None, :],
        mlp_gain[None, :],
        conv_value,
        conv_maps,
    )
    parts = decode(
        peers,
        tokens,
        small,
        jnp.swapaxes(past_value, 0, 1),
        jnp.swapaxes(past_maps, 0, 1),
        (w_gate, w_value, w_maps),
        state,
        (w_out, w_up, w_down),
    )
    layer_out, state_next, tail_v, tail_m = flush(parts)
    return layer_out, state_next, jnp.swapaxes(tail_v, 0, 1), jnp.swapaxes(tail_m, 0, 1)


def kernels_fit(peers, sides, tokens, state, w_maps, w_up):
    rows, part = tokens.shape
    heads = state.shape[1]
    inner = heads * HEAD_DIM
    weights = 2 * tokens.shape[1] * peers * (2 * inner + w_maps.shape[1])
    later = 2 * part * peers * (inner + 2 * w_up.shape[1])
    held = 4 * rows * heads * HEAD_DIM * STATE
    return (
        peers > 1
        and sides == SIDES
        and peers & (peers - 1) == 0
        and rows % 8 == 0
        and 4 * rows <= STATE
        and part % 128 == 0
        and heads % 4 == 0
        and w_maps.shape[1] == heads * 2 * STATE
        and w_up.shape[1] % 128 == 0
        and weights + later <= 44 * 1024 * 1024
        and held <= 12 * 1024 * 1024
    )


def rms_rows(matrix, gain_vec):
    widened = matrix.astype(jnp.float32)
    inv_scale = lax.rsqrt(jnp.mean(widened * widened, axis=-1, keepdims=True) + NORM_EPS)
    return (widened * inv_scale * gain_vec).astype(jnp.bfloat16)


def short_conv(past_rows, newest, kernel):
    window = jnp.concatenate([past_rows, newest[:, None, :]], axis=1)
    summed = jnp.sum(window.astype(jnp.float32) * kernel[None], axis=1)
    return (jax.nn.silu(summed), window[:, 1:, :])


def local(
    tokens,
    mix_gain,
    w_gate,
    w_value,
    w_maps,
    w_step,
    conv_value,
    conv_maps,
    past_value,
    past_maps,
    step_bias,
    decay_log,
    skip_gain,
    head_gain,
    state,
    w_out,
    mlp_gain,
    w_up,
    w_down,
):
    whole_rows = lax.all_gather(tokens, "kv", axis=1, tiled=True)
    batch_rows = whole_rows.shape[0]
    heads_here = state.shape[1]
    head_start = lax.axis_index("kv") * heads_here
    normed = rms_rows(whole_rows, mix_gain)
    gate_pre = jnp.dot(normed, w_gate, preferred_element_type=jnp.float32)
    step_cols = lax.dynamic_slice_in_dim(w_step, head_start, heads_here, 1)
    step_pre = jnp.dot(normed, step_cols, preferred_element_type=jnp.float32)
    value_new = jnp.dot(normed, w_value, preferred_element_type=jnp.float32).astype(jnp.bfloat16)
    maps_new = jnp.dot(normed, w_maps, preferred_element_type=jnp.float32).astype(jnp.bfloat16)
    value_act, value_tail = short_conv(past_value, value_new, conv_value)
    maps_act, maps_tail = short_conv(past_maps, maps_new, conv_maps)
    maps_act = lax.optimization_barrier(maps_act.astype(jnp.bfloat16))
    grouped = maps_act.astype(jnp.float32).reshape(batch_rows, -1, 2, STATE)
    per_group = heads_here // grouped.shape[1]
    in_map = jnp.repeat(grouped[:, :, 0], per_group, axis=1)
    out_map = jnp.repeat(grouped[:, :, 1], per_group, axis=1)
    head_values = value_act.reshape(batch_rows, heads_here, HEAD_DIM)
    step_size = jax.nn.softplus(step_pre + step_bias)
    decay_rate = jnp.exp(-step_size * jnp.exp(decay_log))
    written = (step_size[:, :, None] * head_values)[:, :, :, None] * in_map[:, :, None, :]
    state_next = decay_rate[:, :, None, None] * state + written
    read_out = (
        jnp.sum(state_next * out_map[:, :, None, :], axis=-1)
        + skip_gain[None, :, None] * head_values
    )
    gated_heads = read_out * jax.nn.silu(gate_pre.reshape(batch_rows, heads_here, HEAD_DIM))
    inv_scale = lax.rsqrt(jnp.mean(gated_heads * gated_heads, axis=-1, keepdims=True) + NORM_EPS)
    heads_out = gated_heads * inv_scale * head_gain.reshape(heads_here, HEAD_DIM)
    heads_out = heads_out.reshape(batch_rows, heads_here * HEAD_DIM).astype(jnp.bfloat16)
    partial_value = jnp.dot(heads_out, w_out, preferred_element_type=jnp.float32)
    own_part = lax.psum_scatter(partial_value, "kv", scatter_dimension=1, tiled=True)
    own_hidden = lax.optimization_barrier(
        (tokens.astype(jnp.float32) + own_part).astype(jnp.bfloat16)
    )
    hidden = lax.all_gather(own_hidden, "kv", axis=1, tiled=True)
    normed_mlp = rms_rows(hidden, mlp_gain)
    squared = jnp.square(jax.nn.relu(jnp.dot(normed_mlp, w_up, preferred_element_type=jnp.float32)))
    squared = squared.astype(jnp.bfloat16)
    partial_mlp = jnp.dot(squared, w_down, preferred_element_type=jnp.float32)
    mlp_part = lax.psum_scatter(partial_mlp, "kv", scatter_dimension=1, tiled=True)
    layer_out = (own_hidden.astype(jnp.float32) + mlp_part).astype(jnp.bfloat16)
    return (layer_out, state_next, value_tail, maps_tail)


def solution(mesh):
    in_specs = (
        P(("dp", "tp"), "kv"),
        P(),
        P(None, "kv"),
        P(None, "kv"),
        P(None, "kv"),
        P(),
        P(None, "kv"),
        P(None, "kv"),
        P(("dp", "tp"), None, "kv"),
        P(("dp", "tp"), None, "kv"),
        P("kv"),
        P("kv"),
        P("kv"),
        P("kv"),
        P(("dp", "tp"), "kv", None, None),
        P("kv", None),
        P(),
        P(None, "kv"),
        P("kv", None),
    )
    out_specs = (
        P(("dp", "tp"), "kv"),
        P(("dp", "tp"), "kv", None, None),
        P(("dp", "tp"), None, "kv"),
        P(("dp", "tp"), None, "kv"),
    )
    peers = mesh.shape["kv"]

    def device_part(*args):
        if kernels_fit(peers, mesh.shape["tp"], args[0], args[14], args[4], args[17]):
            return local_kernels(peers, *args)
        return local(*args)

    return jax.shard_map(
        device_part, mesh=mesh, in_specs=in_specs, out_specs=out_specs, check_vma=False
    )
```
